32 devices in a mesh: kv: 8 (over z, y), tp: 4 (over x, core).
Axes of the slice: x: 2, y: 2, z: 4, core: 2. Of those that a mesh axis runs over, the one named last changes fastest.
Arguments:
- tokens: bfloat16 [4, 4096], P(None, 'kv'), may hold values from -70 to 70
- norm_gain: float32 [4096], P('kv'), may hold values from 0.1 to 1.9
- query_weight: bfloat16 [4096, 2048], P('kv', 'tp'), may hold values from -0.09375 to 0.09375
- key_weight: bfloat16 [4096, 256], P('kv', 'tp'), may hold values from -0.09375 to 0.09375
- value_weight: bfloat16 [4096, 256], P('kv', 'tp'), may hold values from -0.09375 to 0.09375
- cache_keys: bfloat16 [4, 2, 6144, 128], P(None, None, ('kv', 'tp')), may hold values from -480 to 480, as said below
- cache_values: bfloat16 [4, 2, 6144, 128], P(None, None, ('kv', 'tp')), may hold values from -6 to 6
- lengths: int32 [4], replicated, may hold values from 1536 to 6143
- lambdas: float32 [16], P('tp'), may hold values from 0.3 to 0.8
- head_gain: float32 [128], replicated, may hold values from 0.1 to 1.9
- output_weight: bfloat16 [2048, 4096], P('tp', 'kv'), may hold values from -0.125 to 0.125
Outputs:
- attended: bfloat16 [4, 4096], P(None, 'kv')
- new_keys: bfloat16 [4, 256], P(None, 'tp')
- new_values: bfloat16 [4, 256], P(None, 'tp')
The draws below stay inside these ranges and needn't reach their ends.
Inputs may be any that keep to these rules, and one draw needn't show every extreme that they name: `cache_keys`: of order 1.75 in most entries; some rows may be far larger.
All inputs are finite; a program needn't handle non-finite values.
Results may differ from the reference program's by a relative error of at most 0.038.
Values may be sent and summed in bfloat16 or wider, within the bound.
No kernel may reach another device: no remote copies, remote signals or barrier semaphores. Data moves between devices by JAX's collectives and lax.ppermute only.
A program may use at most 64 MiB of HBM per device.

```python
import jax
import jax.numpy as jnp
from jax import lax

D = 4096
HEADS = 16
KV_HEADS = 2
QK = 64
VD = 128
SEQS = 4
POSITIONS = 6144
N_TP = 4


def draw_tokens(key, part):
    column = jnp.arange(D, dtype=jnp.float32)
    rising = jnp.exp(jnp.log(4.0) * column / D)
    values = jnp.clip(jax.random.normal(key, (SEQS, D), jnp.float32), -6.0, 6.0) * rising
    return values.astype(jnp.bfloat16)


def draw_cache_keys(key, part):
    drawn = 1.75 * jax.random.normal(key, (SEQS, KV_HEADS, POSITIONS, 2 * QK), jnp.float32)
    return jnp.clip(drawn, -480.0, 480.0).astype(jnp.bfloat16)


def set_ends(values, own_key, least, largest):
    index_at = [jax.random.randint(jax.random.fold_in(own_key, axis), (), 0, length) for axis, length in enumerate(values.shape)]
    widest = values.shape.index(max(values.shape))
    beside = index_at[:widest] + [(index_at[widest] + 1) % values.shape[widest]] + index_at[widest + 1:]
    return values.at[tuple(index_at)].set(least).at[tuple(beside)].set(largest)


def level_of(stream_key, dims, cuts, smallest, top_value):
    def one(dim, blocks):
        steps = jax.random.uniform(jax.random.fold_in(jax.random.fold_in(stream_key, 6), dim), (blocks,), jnp.float32, smallest / len(cuts), top_value / len(cuts))
        return jnp.repeat(jnp.exp(steps), dims[dim] // blocks).reshape((-1,) + (1,) * (len(dims) - dim - 1))

    loudness = one(*cuts[0])
    for cut in cuts[1:]:
        loudness = loudness * one(*cut)
    return loudness


def centred(key, extent, deviation, reach, cuts=(), kind=jnp.bfloat16):
    values = jax.random.normal(key, extent, jnp.float32) * deviation
    if len(cuts) > 0:
        values = level_of(key, extent, cuts, -0.22, 0.18) * values
    return jnp.clip(values, min=-reach, max=reach).astype(kind)


def setup_inputs(seed: int = 0) -> dict:
    seeds = jax.random.split(jax.random.key(seed), 12)
    return {
        "tokens": draw_tokens(jax.random.fold_in(seeds[11], 71), 0),
        "norm_gain": jnp.clip(1.0 + 0.18 * jax.random.normal(seeds[1], (D,), jnp.float32), 0.1, 1.9),
        "query_weight": centred(seeds[2], (D, HEADS * 2 * QK), D ** -0.5, 0.09375, ((0, 8), (1, 4))),
        "key_weight": centred(seeds[3], (D, KV_HEADS * 2 * QK), D ** -0.5, 0.09375, ((0, 8), (1, 4))),
        "value_weight": centred(seeds[4], (D, KV_HEADS * VD), D ** -0.5, 0.09375, ((0, 8), (1, 4))),
        "cache_keys": draw_cache_keys(jax.random.fold_in(seeds[11], 71), 0),
        "cache_values": centred(seeds[6], (SEQS, KV_HEADS, POSITIONS, VD), 1.0, 6.0, ((2, 32),)),
        "lengths": set_ends(jax.random.randint(seeds[7], (SEQS,), POSITIONS // 4, POSITIONS), jax.random.fold_in(seeds[7], 1), POSITIONS // 4, POSITIONS - 1).astype(jnp.int32),
        "lambdas": jnp.clip(0.3 + 0.5 * jax.random.uniform(seeds[8], (HEADS,), jnp.float32) ** level_of(seeds[8], (HEADS,), ((0, 4),), -0.2, 0.2), 0.3, 0.8),
        "head_gain": jnp.clip(1.0 + 0.18 * jax.random.normal(seeds[9], (VD,), jnp.float32), 0.1, 1.9),
        "output_weight": centred(seeds[10], (HEADS * VD, D), (HEADS * VD) ** -0.5, 0.125, ((0, 4), (1, 8))),
    }


NEG_FILL = -1e+30

def reference(tokens, norm_gain, query_weight, key_weight, value_weight, cache_keys, cache_values, lengths, lambdas, head_gain, output_weight):
    floats = tokens.astype(jnp.float32)
    squares = lax.optimization_barrier(jnp.sum(floats * floats, axis=1))
    inverse = lax.rsqrt(squares / D + 1e-06)[:, None]
    scaled = (floats * norm_gain).astype(jnp.bfloat16)
    queries = (jnp.dot(scaled, query_weight, preferred_element_type=jnp.float32) * inverse).astype(jnp.bfloat16)
    new_keys = (jnp.dot(scaled, key_weight, preferred_element_type=jnp.float32) * inverse).astype(jnp.bfloat16)
    new_values = (jnp.dot(scaled, value_weight, preferred_element_type=jnp.float32) * inverse).astype(jnp.bfloat16)
    group_size = HEADS // KV_HEADS
    query_rows = queries.astype(jnp.float32).reshape(SEQS, KV_HEADS, group_size, 2, QK)
    positions = jnp.arange(POSITIONS, dtype=jnp.int32)

    def one_sequence(inputs):
        query_row, key_rows, value_rows, length = inputs
        key_float = key_rows.astype(jnp.float32).reshape(KV_HEADS, POSITIONS, 2, QK)
        scores = jnp.einsum('hgcd,hpcd->hgcp', query_row, key_float) * QK ** (-0.5)
        live_mask = positions < length
        scores = jnp.where(live_mask, scores, NEG_FILL)
        peak = lax.optimization_barrier(jnp.max(scores, axis=-1, keepdims=True))
        weights = jnp.where(live_mask, jnp.exp(scores - peak), 0.0)
        totals = lax.optimization_barrier(jnp.sum(weights, axis=-1))
        rounded = lax.optimization_barrier(weights.astype(jnp.bfloat16)).astype(jnp.float32)
        summed = jnp.einsum('hgcp,hpv->hgcv', rounded, value_rows.astype(jnp.float32))
        return (summed / totals[..., None]).reshape(HEADS, 2, VD)
    ratios = lax.map(one_sequence, (query_rows, cache_keys, cache_values, lengths))
    mixed = ratios[:, :, 0] - lambdas[None, :, None] * ratios[:, :, 1]
    normed = mixed * lax.rsqrt(lax.optimization_barrier(jnp.mean(mixed * mixed, axis=-1, keepdims=True)) + 1e-06) * head_gain
    flattened = normed.astype(jnp.bfloat16).reshape(SEQS, HEADS * VD)
    rows_each = HEADS * VD // N_TP
    attended = jnp.zeros((SEQS, D), jnp.float32)
    for member in range(N_TP):
        partial_out = jnp.dot(flattened[:, member * rows_each:(member + 1) * rows_each], output_weight[member * rows_each:(member + 1) * rows_each], preferred_element_type=jnp.float32)
        attended = attended + lax.optimization_barrier(partial_out.astype(jnp.bfloat16)).astype(jnp.float32)
    return (attended.astype(jnp.bfloat16), new_keys, new_values)
```

```python
import functools

import jax
import jax.numpy as jnp
from jax import lax
from jax.experimental import pallas as pl
from jax.experimental.pallas import tpu as pltpu
from jax.sharding import PartitionSpec as P

HEADS = 16
KV_HEADS = 2
QK = 64
VD = 128
LANES = 128
GROUP = HEADS // KV_HEADS
NEG_FILL = -1e30
VMEM = pl.BlockSpec(memory_space=pltpu.VMEM)
HBM = pl.BlockSpec(memory_space=pltpu.HBM)
PARAMS = pltpu.CompilerParams(vmem_limit_bytes=16 * 1024 * 1024)
CONTRACT_LAST = (((1,), (1,)), ((), ()))


def split3(x):
    high = x.astype(jnp.bfloat16).astype(jnp.float32)
    middle = (x - high).astype(jnp.bfloat16).astype(jnp.float32)
    low = x - high - middle
    return high, middle, low


def lane_of(shape):
    return lax.broadcasted_iota(jnp.int32, shape, 1)


def project(
    tokens_hbm,
    gain_hbm,
    query_hbm,
    key_hbm,
    value_hbm,
    lengths_hbm,
    lambdas_hbm,
    head_gain_hbm,
    send_ref,
    live_ref,
    tail_ref,
    tokens_ref,
    gain_ref,
    query_ref,
    both_ref,
    lengths_ref,
    lambdas_ref,
    head_gain_ref,
    sems,
):
    n_kv, n_tp, seqs, _ = send_ref.shape
    q_cols = query_hbm.shape[1]
    k_cols, v_cols = key_hbm.shape[0], value_hbm.shape[0]
    my_tp = lax.axis_index("tp")
    pairs = (
        (query_hbm, query_ref),
        (tokens_hbm, tokens_ref),
        (gain_hbm, gain_ref),
        (key_hbm, both_ref.at[pl.ds(0, k_cols)]),
        (value_hbm, both_ref.at[pl.ds(k_cols, v_cols)]),
        (lengths_hbm, lengths_ref),
        (lambdas_hbm, lambdas_ref),
        (head_gain_hbm, head_gain_ref),
    )
    copies = [pltpu.make_async_copy(*pair, sems.at[i]) for i, pair in enumerate(pairs)]
    for copy in copies:
        copy.start()
    copies[1].wait()
    copies[2].wait()
    floats = tokens_ref[...].astype(jnp.float32)
    scaled = (floats * gain_ref[...]).astype(jnp.bfloat16)
    squares = jnp.sum(floats * floats, axis=1, keepdims=True)
    lane = lane_of((seqs, LANES))
    high, middle, low = split3(squares)
    squares = jnp.where(lane == 0, high, jnp.where(lane == 1, middle, jnp.where(lane == 2, low, 0.0)))
    copies[3].wait()
    copies[4].wait()
    both = lax.dot_general(scaled, both_ref[...], CONTRACT_LAST, preferred_element_type=jnp.float32)
    if both.shape[1] < LANES:
        both = jnp.concatenate([both, jnp.zeros((seqs, LANES - both.shape[1]), jnp.float32)], axis=1)
    slots = [jnp.where(my_tp == t, both, squares).astype(jnp.bfloat16) for t in range(n_tp)]
    copies[0].wait()
    queries = jnp.dot(scaled, query_ref[...], preferred_element_type=jnp.float32).astype(jnp.bfloat16)

    def fill(v, carry):
        for t in range(n_tp):
            send_ref[v, t, :, :q_cols] = queries
            send_ref[v, t, :, q_cols:] = slots[t]
        return carry

    lax.fori_loop(0, n_kv, fill, 0, unroll=n_kv <= 8)
    for copy in copies[5:]:
        copy.wait()
    pos_count = live_ref.shape[1]
    first_position = (lax.axis_index("kv") * n_tp + my_tp) * pos_count
    positions = first_position + lane_of((1, pos_count))
    for b in range(seqs):
        live_ref[b : b + 1, :] = jnp.where(positions < lengths_ref[b], 1.0, 0.0)
    own_heads = lambdas_ref.shape[0]
    for g in range(own_heads):
        tail_ref[g : g + 1, :] = jnp.full((1, LANES), lambdas_ref[g], jnp.float32)
    tail_ref[own_heads : own_heads + 1, :] = head_gain_ref[...]


def attend(
    width, live_ref, got_ref, keys_ref, values_ref, send_ref, own_ref, q_scr, o_scr, l_scr
):
    n_kv, n_tp, seqs, _ = got_ref.shape
    pos_count = keys_ref.shape[2]
    own_heads = HEADS // n_tp
    q_cols = own_heads * 2 * QK
    my_tp = lax.axis_index("tp")
    other = lax.rem(my_tp + 1, n_tp)

    def add(v, sums):
        parts = [got_ref[v, t, :, :q_cols].astype(jnp.float32) for t in range(n_tp)]
        parts += [got_ref[v, t, :, q_cols:].astype(jnp.float32) for t in (my_tp, other)]
        return tuple(s + p for s, p in zip(sums, parts))

    zero = tuple(jnp.zeros((seqs, q_cols), jnp.float32) for _ in range(n_tp))
    zero += tuple(jnp.zeros((seqs, LANES), jnp.float32) for _ in range(2))
    *totals, both, squares = lax.fori_loop(0, n_kv, add, zero, unroll=n_kv <= 8)
    inverse = lax.rsqrt(jnp.sum(squares, axis=1, keepdims=True) / width + 1e-06)
    own_ref[...] = both * inverse
    for t in range(n_tp):
        queries = (totals[t] * inverse).astype(jnp.bfloat16).astype(jnp.float32)
        for g in range(own_heads):
            head = t * own_heads + g
            q_scr[head * seqs : (head + 1) * seqs, :] = queries[:, g * LANES : (g + 1) * LANES]
    first_map = lane_of((GROUP, LANES)) < QK
    rows = 2 * GROUP
    for b in range(seqs):
        live = jnp.broadcast_to(live_ref[b : b + 1, :], (rows, pos_count)) > 0.0
        for h in range(KV_HEADS):
            q = q_scr[pl.ds(h * GROUP * seqs + b, GROUP, stride=seqs), :]
            q = jnp.concatenate([jnp.where(first_map, q, 0.0), jnp.where(first_map, 0.0, q)], axis=0)
            s = lax.dot_general(
                q.astype(jnp.bfloat16), keys_ref[b, h], CONTRACT_LAST, preferred_element_type=jnp.float32
            )
            s = jnp.where(live, s * QK ** (-0.5), NEG_FILL)
            peak = jnp.max(s, axis=1, keepdims=True)
            e = jnp.where(live, jnp.exp(s - peak), 0.0)
            total = jnp.sum(e, axis=1, keepdims=True)
            o = jnp.dot(e.astype(jnp.bfloat16), values_ref[b, h], preferred_element_type=jnp.float32)
            some = total > 0.0
            total = jnp.where(some, total, 1.0)
            start = (b * KV_HEADS + h) * rows
            o_scr[start : start + rows, :] = o / total
            l_scr[start : start + rows, :] = jnp.broadcast_to(
                jnp.where(some, peak + jnp.log(total), NEG_FILL), (rows, LANES)
            )
    per = 2 * own_heads
    lane = lane_of((seqs, LANES))
    for t in range(n_tp):
        stats = jnp.zeros((seqs, LANES), jnp.float32)
        for j in range(per):
            head = t * own_heads + j // 2
            start = (head // GROUP) * rows + (j % 2) * GROUP + head % GROUP
            from_seqs = pl.ds(start, seqs, stride=KV_HEADS * rows)
            o = o_scr[from_seqs, :].astype(jnp.bfloat16)
            for part, value in enumerate(split3(l_scr[from_seqs, :])):
                stats = jnp.where(lane == part * per + j, value, stats)
            for v in range(n_kv):
                send_ref[v, t, :, j * VD : (j + 1) * VD] = o
        stats = stats.astype(jnp.bfloat16)
        for v in range(n_kv):
            send_ref[v, t, :, per * VD :] = stats


def finish(tail_ref, got_ref, weight_ref, out_ref):
    count, seqs, _ = got_ref.shape
    own_heads = tail_ref.shape[0] - 1
    per = 2 * own_heads

    def logs_of(d):
        stats = got_ref[d, :, per * VD :].astype(jnp.float32)
        return stats + pltpu.roll(stats, LANES - per, 1) + pltpu.roll(stats, LANES - 2 * per, 1)

    unroll = count <= 32
    peak = lax.fori_loop(1, count, lambda d, m: jnp.maximum(m, logs_of(d)), logs_of(0), unroll=unroll)

    def add(d, carry):
        total, *sums = carry
        share = jnp.exp(logs_of(d) - peak)
        for j in range(per):
            sums[j] = sums[j] + share[:, j : j + 1] * got_ref[d, :, j * VD : (j + 1) * VD].astype(jnp.float32)
        return (total + share, *sums)

    zero = tuple(jnp.zeros((seqs, LANES), jnp.float32) for _ in range(per + 1))
    total, *sums = lax.fori_loop(0, count, add, zero, unroll=unroll)
    inverse = 1.0 / total
    ratios = [sums[j] * inverse[:, j : j + 1] for j in range(per)]
    heads = []
    for g in range(own_heads):
        mixed = ratios[2 * g] - tail_ref[g : g + 1, :] * ratios[2 * g + 1]
        scale = lax.rsqrt(jnp.mean(mixed * mixed, axis=1, keepdims=True) + 1e-06)
        heads.append((mixed * scale * tail_ref[own_heads : own_heads + 1, :]).astype(jnp.bfloat16))
    flattened = jnp.concatenate(heads, axis=1)
    out_ref[...] = jnp.dot(flattened, weight_ref[...], preferred_element_type=jnp.float32).astype(jnp.bfloat16)


def body(
    tokens,
    norm_gain,
    query_weight,
    key_weight,
    value_weight,
    cache_keys,
    cache_values,
    lengths,
    lambdas,
    head_gain,
    output_weight,
):
    n_kv, n_tp = lax.axis_size("kv"), lax.axis_size("tp")
    everyone = ("kv", "tp")
    seqs = tokens.shape[0]
    own_heads = lambdas.shape[0]
    q_cols = query_weight.shape[1]
    k_cols, v_cols = key_weight.shape[1], value_weight.shape[1]
    pos_count = cache_keys.shape[2]
    width = tokens.shape[1] * n_kv
    first = q_cols + LANES
    send, live, tail = pl.pallas_call(
        project,
        out_shape=(
            jax.ShapeDtypeStruct((n_kv, n_tp, seqs, first), jnp.bfloat16),
            jax.ShapeDtypeStruct((seqs, pos_count), jnp.float32),
            jax.ShapeDtypeStruct((own_heads + 1, LANES), jnp.float32),
        ),
        in_specs=[HBM] * 8,
        out_specs=(VMEM, VMEM, VMEM),
        scratch_shapes=[
            pltpu.VMEM(tokens.shape, tokens.dtype),
            pltpu.VMEM((1, tokens.shape[1]), jnp.float32),
            pltpu.VMEM(query_weight.shape, query_weight.dtype),
            pltpu.VMEM((k_cols + v_cols, tokens.shape[1]), key_weight.dtype),
            pltpu.SMEM(lengths.shape, lengths.dtype),
            pltpu.SMEM(lambdas.shape, lambdas.dtype),
            pltpu.VMEM((1, LANES), jnp.float32),
            pltpu.SemaphoreType.DMA((8,)),
        ],
        compiler_params=PARAMS,
    )(
        *(
            pltpu.with_memory_space_constraint(x, pltpu.HBM)
            for x in (
                tokens,
                norm_gain[None],
                query_weight,
                key_weight.T,
                value_weight.T,
                lengths,
                lambdas,
                head_gain[None],
            )
        )
    )
    got = lax.all_to_all(send.reshape(n_kv * n_tp, seqs, first), everyone, 0, 0, tiled=True)
    second = 2 * own_heads * VD + LANES
    rows = seqs * HEADS * 2
    send, own = pl.pallas_call(
        functools.partial(attend, width),
        out_shape=(
            jax.ShapeDtypeStruct((n_kv, n_tp, seqs, second), jnp.bfloat16),
            jax.ShapeDtypeStruct((seqs, LANES), jnp.float32),
        ),
        in_specs=[VMEM] * 4,
        out_specs=(VMEM, VMEM),
        compiler_params=PARAMS,
        scratch_shapes=[
            pltpu.VMEM((HEADS * seqs, LANES), jnp.float32),
            pltpu.VMEM((rows, LANES), jnp.float32),
            pltpu.VMEM((rows, LANES), jnp.float32),
        ],
    )(live, got.reshape(n_kv, n_tp, seqs, first), cache_keys, cache_values)
    got = lax.all_to_all(send.reshape(n_kv * n_tp, seqs, second), everyone, 0, 0, tiled=True)
    got, own = lax.optimization_barrier((got, own))
    new_keys = own[:, :k_cols].astype(jnp.bfloat16)
    new_values = own[:, k_cols : k_cols + v_cols].astype(jnp.bfloat16)
    partial_out = pl.pallas_call(
        finish,
        out_shape=jax.ShapeDtypeStruct((seqs, output_weight.shape[1]), jnp.bfloat16),
        in_specs=[VMEM] * 3,
        out_specs=VMEM,
        compiler_params=PARAMS,
    )(tail, got, output_weight)
    out = partial_out.astype(jnp.float32)
    for step in range(1, n_tp):
        out = out + lax.ppermute(partial_out, "tp", [(i, i ^ step) for i in range(n_tp)]).astype(jnp.float32)
    return (out.astype(jnp.bfloat16), new_keys, new_values)


def solution(mesh):
    return jax.shard_map(
        body,
        mesh=mesh,
        in_specs=(
            P(None, "kv"),
            P("kv"),
            P("kv", "tp"),
            P("kv", "tp"),
            P("kv", "tp"),
            P(None, None, ("kv", "tp"), None),
            P(None, None, ("kv", "tp"), None),
            P(),
            P("tp"),
            P(),
            P("tp", "kv"),
        ),
        out_specs=(P(None, "kv"), P(None, "tp"), P(None, "tp")),
        check_vma=False,
    )
```

```python
import functools

import jax
import jax.numpy as jnp
from jax import lax
from jax.experimental import pallas as pl
from jax.experimental.pallas import tpu as pltpu
from jax.sharding import PartitionSpec as P

HEADS = 16
KV_HEADS = 2
QK = 64
VD = 128
LANES = 128
GROUP = HEADS // KV_HEADS
NEG_FILL = -1e30
VMEM = pl.BlockSpec(memory_space=pltpu.VMEM)
HBM = pl.BlockSpec(memory_space=pltpu.HBM)
PARAMS = pltpu.CompilerParams(vmem_limit_bytes=16 * 1024 * 1024)
SCALE = 8.0
BASE = 2048.0
PARTS = 5
CONTRACT_LAST = (((1,), (1,)), ((), ()))


def split3(x):
    high = x.astype(jnp.bfloat16).astype(jnp.float32)
    middle = (x - high).astype(jnp.bfloat16).astype(jnp.float32)
    low = x - high - middle
    return high, middle, low


def lane_of(shape):
    return lax.broadcasted_iota(jnp.int32, shape, 1)


def project(
    width,
    tokens_hbm,
    gain_hbm,
    query_hbm,
    key_hbm,
    value_hbm,
    lengths_hbm,
    lambdas_hbm,
    head_gain_hbm,
    send_ref,
    live_ref,
    tail_ref,
    tokens_ref,
    gain_ref,
    query_ref,
    both_ref,
    lengths_ref,
    lambdas_ref,
    head_gain_ref,
    sems,
):
    n_tp, half, _ = send_ref.shape
    seqs = tokens_hbm.shape[0]
    q_cols = query_hbm.shape[1]
    k_cols, v_cols = key_hbm.shape[0], value_hbm.shape[0]
    my_tp = lax.axis_index("tp")
    pairs = (
        (query_hbm, query_ref),
        (tokens_hbm, tokens_ref),
        (gain_hbm, gain_ref),
        (key_hbm, both_ref.at[pl.ds(0, k_cols)]),
        (value_hbm, both_ref.at[pl.ds(k_cols, v_cols)]),
        (lengths_hbm, lengths_ref),
        (lambdas_hbm, lambdas_ref),
        (head_gain_hbm, head_gain_ref),
    )
    copies = [pltpu.make_async_copy(*pair, sems.at[i]) for i, pair in enumerate(pairs)]
    for copy in copies:
        copy.start()
    copies[1].wait()
    copies[2].wait()
    floats = tokens_ref[...].astype(jnp.float32)
    scaled = (floats * gain_ref[...]).astype(jnp.bfloat16)
    squares = jnp.sum(floats * floats, axis=1, keepdims=True)
    lane = lane_of((seqs, LANES))
    rest = squares * (1.0 / width)
    squares = jnp.zeros((seqs, LANES), jnp.float32)
    for part in range(PARTS):
        digit = jnp.floor(rest)
        squares = jnp.where(lane == part, digit, squares)
        rest = (rest - digit) * BASE
    copies[3].wait()
    copies[4].wait()
    both = lax.dot_general(scaled, both_ref[...], CONTRACT_LAST, preferred_element_type=jnp.float32)
    if both.shape[1] < LANES:
        both = jnp.concatenate([both, jnp.zeros((seqs, LANES - both.shape[1]), jnp.float32)], axis=1)
    both, squares = (jnp.concatenate([x[:half], x[half:]], axis=1) for x in (both * SCALE, squares))
    copies[0].wait()
    queries = jnp.dot(scaled, query_ref[...], preferred_element_type=jnp.float32) * SCALE
    for t in range(n_tp):
        send_ref[t, :, :q_cols] = queries[half:] if t % 2 else queries[:half]
        send_ref[t, :, q_cols:] = jnp.where(my_tp == t, both, squares)
    for copy in copies[5:]:
        copy.wait()
    pos_count = live_ref.shape[1]
    core = lax.rem(my_tp, 2)
    own_block = lax.axis_index("kv") * n_tp + my_tp
    lane = lane_of((1, pos_count))
    for side, block in enumerate((own_block, own_block + 1 - 2 * core)):
        positions = block * pos_count + lane
        for b in range(half):
            row = side * half + b
            live_ref[row : row + 1, :] = jnp.where(positions < lengths_ref[core * half + b], 1.0, 0.0)
    own_heads = lambdas_ref.shape[0]
    for g in range(own_heads):
        tail_ref[g : g + 1, :] = jnp.full((1, LANES), lambdas_ref[g], jnp.float32)
    tail_ref[own_heads : own_heads + 1, :] = head_gain_ref[...]


def attend(
    live_ref,
    got_ref,
    keys_ref,
    values_ref,
    pair_keys_ref,
    pair_values_ref,
    send_ref,
    own_ref,
    q_scr,
    o_scr,
    l_scr,
):
    n_kv, n_tp, half, _ = send_ref.shape
    pos_count = keys_ref.shape[2]
    own_heads = HEADS // n_tp
    q_cols = own_heads * 2 * QK
    my_tp = lax.axis_index("tp")
    core = lax.rem(my_tp, 2)
    lane = lane_of((half, LANES))
    weight = jnp.zeros((half, LANES), jnp.float32)
    for part in range(PARTS):
        weight = jnp.where(lane == part, BASE**-part, weight)
    inverses = []
    for c in range(2):
        lanes = slice(q_cols + c * LANES, q_cols + (c + 1) * LANES)
        squares = jnp.sum(got_ref[lax.rem(my_tp + 1, n_tp), :, lanes] * weight, axis=1, keepdims=True)
        inverses.append(lax.rsqrt(squares + 1e-06) * (1.0 / SCALE))
        own_ref[c * half : (c + 1) * half, :] = got_ref[my_tp, :, lanes] * inverses[c]
    inverse = jnp.where(core == 0, inverses[0], inverses[1])
    for t in range(n_tp):
        queries = (got_ref[t, :, :q_cols] * inverse).astype(jnp.bfloat16).astype(jnp.float32)
        for g in range(own_heads):
            head = t * own_heads + g
            q_scr[head * half : (head + 1) * half, :] = queries[:, g * LANES : (g + 1) * LANES]
    first_map = lane_of((GROUP, LANES)) < QK
    rows = 2 * GROUP
    for b in range(half):
        seq = core * half + b
        lives = [
            jnp.broadcast_to(live_ref[side * half + b : side * half + b + 1, :], (rows, pos_count)) > 0.0
            for side in range(2)
        ]
        for h in range(KV_HEADS):
            q = q_scr[pl.ds(h * GROUP * half + b, GROUP, stride=half), :]
            q = jnp.concatenate([jnp.where(first_map, q, 0.0), jnp.where(first_map, 0.0, q)], axis=0)
            q = q.astype(jnp.bfloat16)
            scores = [
                jnp.where(
                    live,
                    lax.dot_general(q, ref[seq, h], CONTRACT_LAST, preferred_element_type=jnp.float32) * QK ** (-0.5),
                    NEG_FILL,
                )
                for live, ref in zip(lives, (keys_ref, pair_keys_ref))
            ]
            peak = jnp.maximum(*(jnp.max(s, axis=1, keepdims=True) for s in scores))
            weights = [jnp.where(live, jnp.exp(s - peak), 0.0) for live, s in zip(lives, scores)]
            total = jnp.sum(weights[0], axis=1, keepdims=True) + jnp.sum(weights[1], axis=1, keepdims=True)
            o = sum(
                jnp.dot(e.astype(jnp.bfloat16), ref[seq, h], preferred_element_type=jnp.float32)
                for e, ref in zip(weights, (values_ref, pair_values_ref))
            )
            some = total > 0.0
            total = jnp.where(some, total, 1.0)
            start = (b * KV_HEADS + h) * rows
            o_scr[start : start + rows, :] = o / total
            l_scr[start : start + rows, :] = jnp.broadcast_to(
                jnp.where(some, peak + jnp.log(total), NEG_FILL), (rows, LANES)
            )
    per = 2 * own_heads
    lane = lane_of((half, LANES))
    for t in range(n_tp):
        stats = jnp.zeros((half, LANES), jnp.float32)
        for j in range(per):
            head = t * own_heads + j // 2
            start = (head // GROUP) * rows + (j % 2) * GROUP + head % GROUP
            from_seqs = pl.ds(start, half, stride=KV_HEADS * rows)
            o = o_scr[from_seqs, :].astype(jnp.bfloat16)
            for part, value in enumerate(split3(l_scr[from_seqs, :])):
                stats = jnp.where(lane == part * per + j, value, stats)
            for v in range(n_kv):
                send_ref[v, t, :, j * VD : (j + 1) * VD] = o
        stats = stats.astype(jnp.bfloat16)
        for v in range(n_kv):
            send_ref[v, t, :, per * VD :] = stats


def finish(tail_ref, got_ref, weight_ref, out_ref):
    count, half, _ = got_ref.shape
    own_heads = tail_ref.shape[0] - 1
    per = 2 * own_heads

    def logs_of(d):
        stats = got_ref[d, :, per * VD :].astype(jnp.float32)
        return stats + pltpu.roll(stats, LANES - per, 1) + pltpu.roll(stats, LANES - 2 * per, 1)

    parts = []
    for core in range(2):

        def peak_of(d, peak, core=core):
            return jnp.maximum(peak, logs_of(2 * d + core))

        def add(d, carry, core=core):
            total, *sums = carry
            share = jnp.exp(logs_of(2 * d + core) - peak)
            for j in range(per):
                got = got_ref[2 * d + core, :, j * VD : (j + 1) * VD].astype(jnp.float32)
                sums[j] = sums[j] + share[:, j : j + 1] * got
            return (total + share, *sums)

        unroll = count <= 32
        peak = lax.fori_loop(1, count // 2, peak_of, logs_of(core), unroll=unroll)
        zero = tuple(jnp.zeros((half, LANES), jnp.float32) for _ in range(per + 1))
        parts.append(lax.fori_loop(0, count // 2, add, zero, unroll=unroll))
    total, *sums = (jnp.concatenate(pair, axis=0) for pair in zip(*parts))
    inverse = 1.0 / total
    ratios = [sums[j] * inverse[:, j : j + 1] for j in range(per)]
    heads = []
    for g in range(own_heads):
        mixed = ratios[2 * g] - tail_ref[g : g + 1, :] * ratios[2 * g + 1]
        scale = lax.rsqrt(jnp.mean(mixed * mixed, axis=1, keepdims=True) + 1e-06)
        heads.append((mixed * scale * tail_ref[own_heads : own_heads + 1, :]).astype(jnp.bfloat16))
    flattened = jnp.concatenate(heads, axis=1)
    out_ref[...] = jnp.dot(flattened, weight_ref[...], preferred_element_type=jnp.float32).astype(jnp.bfloat16)


def body(
    tokens,
    norm_gain,
    query_weight,
    key_weight,
    value_weight,
    cache_keys,
    cache_values,
    lengths,
    lambdas,
    head_gain,
    output_weight,
):
    n_kv, n_tp = lax.axis_size("kv"), lax.axis_size("tp")
    everyone = ("kv", "tp")
    seqs = tokens.shape[0]
    half = seqs // 2
    own_heads = lambdas.shape[0]
    q_cols = query_weight.shape[1]
    k_cols, v_cols = key_weight.shape[1], value_weight.shape[1]
    pos_count = cache_keys.shape[2]
    width = tokens.shape[1] * n_kv
    cores = [(i, i ^ 1) for i in range(n_tp)]
    pair_keys = lax.ppermute(cache_keys, "tp", cores)
    pair_values = lax.ppermute(cache_values, "tp", cores)
    first = q_cols + 2 * LANES
    send, live, tail = pl.pallas_call(
        functools.partial(project, width),
        out_shape=(
            jax.ShapeDtypeStruct((n_tp, half, first), jnp.float32),
            jax.ShapeDtypeStruct((seqs, pos_count), jnp.float32),
            jax.ShapeDtypeStruct((own_heads + 1, LANES), jnp.float32),
        ),
        in_specs=[HBM] * 8,
        out_specs=(VMEM, VMEM, VMEM),
        scratch_shapes=[
            pltpu.VMEM(tokens.shape, tokens.dtype),
            pltpu.VMEM((1, tokens.shape[1]), jnp.float32),
            pltpu.VMEM(query_weight.shape, query_weight.dtype),
            pltpu.VMEM((k_cols + v_cols, tokens.shape[1]), key_weight.dtype),
            pltpu.SMEM(lengths.shape, lengths.dtype),
            pltpu.SMEM(lambdas.shape, lambdas.dtype),
            pltpu.VMEM((1, LANES), jnp.float32),
            pltpu.SemaphoreType.DMA((8,)),
        ],
        compiler_params=PARAMS,
    )(
        *(
            pltpu.with_memory_space_constraint(x, pltpu.HBM)
            for x in (
                tokens,
                norm_gain[None],
                query_weight,
                key_weight.T,
                value_weight.T,
                lengths,
                lambdas,
                head_gain[None],
            )
        )
    )
    send = jnp.broadcast_to(send.astype(jnp.float16)[None], (n_kv, n_tp, half, first))
    got = lax.all_to_all(send.reshape(n_kv * n_tp, half, first), everyone, 0, 0, tiled=True)
    got = jnp.sum(got.reshape(n_kv, n_tp, half, first).astype(jnp.float32), axis=0)
    second = 2 * own_heads * VD + LANES
    rows = half * HEADS * 2
    send, own = pl.pallas_call(
        attend,
        out_shape=(
            jax.ShapeDtypeStruct((n_kv, n_tp, half, second), jnp.bfloat16),
            jax.ShapeDtypeStruct((seqs, LANES), jnp.float32),
        ),
        in_specs=[VMEM] * 6,
        out_specs=(VMEM, VMEM),
        compiler_params=PARAMS,
        scratch_shapes=[
            pltpu.VMEM((HEADS * half, LANES), jnp.float32),
            pltpu.VMEM((rows, LANES), jnp.float32),
            pltpu.VMEM((rows, LANES), jnp.float32),
        ],
    )(live, got, cache_keys, cache_values, pair_keys, pair_values)
    got = lax.all_to_all(send.reshape(n_kv * n_tp, half, second), everyone, 0, 0, tiled=True)
    got, own = lax.optimization_barrier((got, own))
    new_keys = own[:, :k_cols].astype(jnp.bfloat16)
    new_values = own[:, k_cols : k_cols + v_cols].astype(jnp.bfloat16)
    partial_out = pl.pallas_call(
        finish,
        out_shape=jax.ShapeDtypeStruct((seqs, output_weight.shape[1]), jnp.bfloat16),
        in_specs=[VMEM] * 3,
        out_specs=VMEM,
        compiler_params=PARAMS,
    )(tail, got, output_weight)
    out = partial_out.astype(jnp.float32)
    for step in range(1, n_tp):
        out = out + lax.ppermute(partial_out, "tp", [(i, i ^ step) for i in range(n_tp)]).astype(jnp.float32)
    return (out.astype(jnp.bfloat16), new_keys, new_values)


def solution(mesh):
    return jax.shard_map(
        body,
        mesh=mesh,
        in_specs=(
            P(None, "kv"),
            P("kv"),
            P("kv", "tp"),
            P("kv", "tp"),
            P("kv", "tp"),
            P(None, None, ("kv", "tp"), None),
            P(None, None, ("kv", "tp"), None),
            P(),
            P("tp"),
            P(),
            P("tp", "kv"),
        ),
        out_specs=(P(None, "kv"), P(None, "tp"), P(None, "tp")),
        check_vma=False,
    )
```

```python
import functools

import jax
import jax.numpy as jnp
from jax import lax
from jax.experimental import pallas as pl
from jax.experimental.pallas import tpu as pltpu
from jax.sharding import PartitionSpec as P

HEADS = 16
KV_HEADS = 2
QK = 64
VD = 128
LANES = 128
GROUP = HEADS // KV_HEADS
NEG_FILL = -1e30
VMEM = pl.BlockSpec(memory_space=pltpu.VMEM)
HBM = pl.BlockSpec(memory_space=pltpu.HBM)
PARAMS = pltpu.CompilerParams(vmem_limit_bytes=16 * 1024 * 1024)
SQUARES_AT = 96
OWN_AT = 64
CONTRACT_LAST = (((1,), (1,)), ((), ()))


def split3(x):
    high = x.astype(jnp.bfloat16).astype(jnp.float32)
    middle = (x - high).astype(jnp.bfloat16).astype(jnp.float32)
    low = x - high - middle
    return high, middle, low


def lane_of(shape):
    return lax.broadcasted_iota(jnp.int32, shape, 1)


def for_each(count, step):
    if count <= 8:
        for i in range(count):
            step(i)
    else:
        lax.fori_loop(0, count, lambda i, _: step(i), None)


def shifted(x, by):
    return pltpu.roll(x, lax.rem(by + 2 * LANES, LANES) if not isinstance(by, int) else by % LANES, 1)


def project(
    tokens_hbm,
    gain_hbm,
    query_hbm,
    key_hbm,
    value_hbm,
    lengths_hbm,
    lambdas_hbm,
    head_gain_hbm,
    send_ref,
    live_ref,
    tail_ref,
    tokens_ref,
    gain_ref,
    query_ref,
    both_ref,
    lengths_ref,
    lambdas_ref,
    head_gain_ref,
    sems,
):
    n_kv, n_tp, half, _ = send_ref.shape
    seqs = tokens_hbm.shape[0]
    q_cols = query_hbm.shape[1]
    k_cols, v_cols = key_hbm.shape[0], value_hbm.shape[0]
    my_tp = lax.axis_index("tp")
    pairs = (
        (query_hbm, query_ref),
        (tokens_hbm, tokens_ref),
        (gain_hbm, gain_ref),
        (key_hbm, both_ref.at[pl.ds(0, k_cols)]),
        (value_hbm, both_ref.at[pl.ds(k_cols, v_cols)]),
        (lengths_hbm, lengths_ref),
        (lambdas_hbm, lambdas_ref),
        (head_gain_hbm, head_gain_ref),
    )
    copies = [pltpu.make_async_copy(*pair, sems.at[i]) for i, pair in enumerate(pairs)]
    for copy in copies:
        copy.start()
    copies[1].wait()
    copies[2].wait()
    floats = tokens_ref[...].astype(jnp.float32)
    scaled = (floats * gain_ref[...]).astype(jnp.bfloat16)
    squares = jnp.sum(floats * floats, axis=1, keepdims=True)
    copies[3].wait()
    copies[4].wait()
    both = lax.dot_general(scaled, both_ref[...], CONTRACT_LAST, preferred_element_type=jnp.float32)
    if both.shape[1] < LANES:
        both = jnp.concatenate([both, jnp.zeros((seqs, LANES - both.shape[1]), jnp.float32)], axis=1)
    lane = lane_of((half, LANES))
    squares = jnp.where(lane == SQUARES_AT, squares[:half], squares[half:])
    piece = (k_cols + v_cols) // n_kv
    copies[0].wait()
    queries = jnp.dot(scaled, query_ref[...], preferred_element_type=jnp.float32)

    def fill(v):
        slot = jnp.where(lane < 2 * piece, shifted(both[half:], piece - v * piece), squares)
        slot = jnp.where(lane < piece, shifted(both[:half], -v * piece), slot)
        for t in range(n_tp):
            send_ref[v, t, :, :q_cols] = queries[half:] if t % 2 else queries[:half]
            send_ref[v, t, :, q_cols:] = slot

    for_each(n_kv, fill)
    for copy in copies[5:]:
        copy.wait()
    pos_count = live_ref.shape[1]
    core = lax.rem(my_tp, 2)
    own_block = lax.axis_index("kv") * n_tp + my_tp
    lane = lane_of((1, pos_count))
    for side, block in enumerate((own_block, own_block + 1 - 2 * core)):
        positions = block * pos_count + lane
        for b in range(half):
            row = side * half + b
            live_ref[row : row + 1, :] = jnp.where(positions < lengths_ref[core * half + b], 1.0, 0.0)
    own_heads = lambdas_ref.shape[0]
    for g in range(own_heads):
        tail_ref[g : g + 1, :] = jnp.full((1, LANES), lambdas_ref[g], jnp.float32)
    tail_ref[own_heads : own_heads + 1, :] = head_gain_ref[...]


def attend(
    width,
    piece,
    live_ref,
    got_ref,
    keys_ref,
    values_ref,
    pair_keys_ref,
    pair_values_ref,
    send_ref,
    q_scr,
    o_scr,
    l_scr,
):
    n_kv, n_tp, half, _ = send_ref.shape
    pos_count = keys_ref.shape[2]
    own_heads = HEADS // n_tp
    q_cols = own_heads * 2 * QK
    my_tp = lax.axis_index("tp")
    core = lax.rem(my_tp, 2)

    def add(v, sums):
        parts = [got_ref[v, t, :, :q_cols] for t in range(n_tp)] + [got_ref[v, my_tp, :, q_cols:]]
        return tuple(s + p for s, p in zip(sums, parts))

    zero = tuple(jnp.zeros((half, q_cols), jnp.float32) for _ in range(n_tp)) + (jnp.zeros((half, LANES), jnp.float32),)
    *totals, slot = lax.fori_loop(0, n_kv, add, zero, unroll=n_kv <= 8)
    inverses = [
        lax.rsqrt(slot[:, at : at + 1] / width + 1e-06) for at in (SQUARES_AT, SQUARES_AT + 1)
    ]
    inverse = jnp.where(core == 0, inverses[0], inverses[1])
    lane = lane_of((half, LANES))
    own = shifted(slot * jnp.where(lane < piece, inverses[0], inverses[1]), OWN_AT)
    for t in range(n_tp):
        queries = (totals[t] * inverse).astype(jnp.bfloat16).astype(jnp.float32)
        for g in range(own_heads):
            head = t * own_heads + g
            q_scr[head * half : (head + 1) * half, :] = queries[:, g * LANES : (g + 1) * LANES]
    first_map = lane_of((GROUP, LANES)) < QK
    rows = 2 * GROUP
    for b in range(half):
        seq = core * half + b
        lives = [
            jnp.broadcast_to(live_ref[side * half + b : side * half + b + 1, :], (rows, pos_count)) > 0.0
            for side in range(2)
        ]
        for h in range(KV_HEADS):
            q = q_scr[pl.ds(h * GROUP * half + b, GROUP, stride=half), :]
            q = jnp.concatenate([jnp.where(first_map, q, 0.0), jnp.where(first_map, 0.0, q)], axis=0)
            q = q.astype(jnp.bfloat16)
            scores = [
                jnp.where(
                    live,
                    lax.dot_general(q, ref[seq, h], CONTRACT_LAST, preferred_element_type=jnp.float32) * QK ** (-0.5),
                    NEG_FILL,
                )
                for live, ref in zip(lives, (keys_ref, pair_keys_ref))
            ]
            peak = jnp.maximum(*(jnp.max(s, axis=1, keepdims=True) for s in scores))
            weights = [jnp.where(live, jnp.exp(s - peak), 0.0) for live, s in zip(lives, scores)]
            total = jnp.sum(weights[0], axis=1, keepdims=True) + jnp.sum(weights[1], axis=1, keepdims=True)
            o = sum(
                jnp.dot(e.astype(jnp.bfloat16), ref[seq, h], preferred_element_type=jnp.float32)
                for e, ref in zip(weights, (values_ref, pair_values_ref))
            )
            some = total > 0.0
            total = jnp.where(some, total, 1.0)
            start = (b * KV_HEADS + h) * rows
            o_scr[start : start + rows, :] = o / total
            l_scr[start : start + rows, :] = jnp.broadcast_to(
                jnp.where(some, peak + jnp.log(total), NEG_FILL), (rows, LANES)
            )
    per = 2 * own_heads
    for t in range(n_tp):
        stats = own
        for j in range(per):
            head = t * own_heads + j // 2
            start = (head // GROUP) * rows + (j % 2) * GROUP + head % GROUP
            from_seqs = pl.ds(start, half, stride=KV_HEADS * rows)
            o = o_scr[from_seqs, :].astype(jnp.bfloat16)
            for part, value in enumerate(split3(l_scr[from_seqs, :])):
                stats = jnp.where(lane == part * per + j, value, stats)
            for v in range(n_kv):
                send_ref[v, t, :, j * VD : (j + 1) * VD] = o
        stats = stats.astype(jnp.bfloat16)
        for v in range(n_kv):
            send_ref[v, t, :, per * VD :] = stats


def finish(n_tp, piece, tail_ref, got_ref, weight_ref, out_ref, own_ref):
    count, half, _ = got_ref.shape
    own_heads = tail_ref.shape[0] - 1
    per = 2 * own_heads

    def logs_of(d):
        stats = got_ref[d, :, per * VD :].astype(jnp.float32)
        return stats + pltpu.roll(stats, LANES - per, 1) + pltpu.roll(stats, LANES - 2 * per, 1)

    lane = lane_of((half, LANES))
    for c in range(2):
        own_ref[c * half : (c + 1) * half, :] = jnp.zeros((half, LANES), jnp.float32)

    def collect(v):
        slot = got_ref[v * n_tp + lax.axis_index("tp"), :, per * VD :].astype(jnp.float32)
        inside = (lane >= v * piece) & (lane < (v + 1) * piece)
        for c in range(2):
            rows = slice(c * half, (c + 1) * half)
            own_ref[rows, :] = jnp.where(inside, shifted(slot, v * piece - OWN_AT - c * piece), own_ref[rows, :])

    for_each(count // n_tp, collect)
    parts = []
    for core in range(2):

        def peak_of(d, peak, core=core):
            return jnp.maximum(peak, logs_of(2 * d + core))

        def add(d, carry, core=core):
            total, *sums = carry
            share = jnp.exp(logs_of(2 * d + core) - peak)
            for j in range(per):
                got = got_ref[2 * d + core, :, j * VD : (j + 1) * VD].astype(jnp.float32)
                sums[j] = sums[j] + share[:, j : j + 1] * got
            return (total + share, *sums)

        unroll = count <= 32
        peak = lax.fori_loop(1, count // 2, peak_of, logs_of(core), unroll=unroll)
        zero = tuple(jnp.zeros((half, LANES), jnp.float32) for _ in range(per + 1))
        parts.append(lax.fori_loop(0, count // 2, add, zero, unroll=unroll))
    total, *sums = (jnp.concatenate(pair, axis=0) for pair in zip(*parts))
    inverse = 1.0 / total
    ratios = [sums[j] * inverse[:, j : j + 1] for j in range(per)]
    heads = []
    for g in range(own_heads):
        mixed = ratios[2 * g] - tail_ref[g : g + 1, :] * ratios[2 * g + 1]
        scale = lax.rsqrt(jnp.mean(mixed * mixed, axis=1, keepdims=True) + 1e-06)
        heads.append((mixed * scale * tail_ref[own_heads : own_heads + 1, :]).astype(jnp.bfloat16))
    flattened = jnp.concatenate(heads, axis=1)
    out_ref[...] = jnp.dot(flattened, weight_ref[...], preferred_element_type=jnp.float32).astype(jnp.bfloat16)


def body(
    tokens,
    norm_gain,
    query_weight,
    key_weight,
    value_weight,
    cache_keys,
    cache_values,
    lengths,
    lambdas,
    head_gain,
    output_weight,
):
    n_kv, n_tp = lax.axis_size("kv"), lax.axis_size("tp")
    everyone = ("kv", "tp")
    seqs = tokens.shape[0]
    half = seqs // 2
    own_heads = lambdas.shape[0]
    q_cols = query_weight.shape[1]
    k_cols, v_cols = key_weight.shape[1], value_weight.shape[1]
    pos_count = cache_keys.shape[2]
    width = tokens.shape[1] * n_kv
    cores = [(i, i ^ 1) for i in range(n_tp)]
    pair_keys = lax.ppermute(cache_keys, "tp", cores)
    pair_values = lax.ppermute(cache_values, "tp", cores)
    first = q_cols + LANES
    piece = (k_cols + v_cols) // n_kv
    send, live, tail = pl.pallas_call(
        project,
        out_shape=(
            jax.ShapeDtypeStruct((n_kv, n_tp, half, first), jnp.float32),
            jax.ShapeDtypeStruct((seqs, pos_count), jnp.float32),
            jax.ShapeDtypeStruct((own_heads + 1, LANES), jnp.float32),
        ),
        in_specs=[HBM] * 8,
        out_specs=(VMEM, VMEM, VMEM),
        scratch_shapes=[
            pltpu.VMEM(tokens.shape, tokens.dtype),
            pltpu.VMEM((1, tokens.shape[1]), jnp.float32),
            pltpu.VMEM(query_weight.shape, query_weight.dtype),
            pltpu.VMEM((k_cols + v_cols, tokens.shape[1]), key_weight.dtype),
            pltpu.SMEM(lengths.shape, lengths.dtype),
            pltpu.SMEM(lambdas.shape, lambdas.dtype),
            pltpu.VMEM((1, LANES), jnp.float32),
            pltpu.SemaphoreType.DMA((8,)),
        ],
        compiler_params=PARAMS,
    )(
        *(
            pltpu.with_memory_space_constraint(x, pltpu.HBM)
            for x in (
                tokens,
                norm_gain[None],
                query_weight,
                key_weight.T,
                value_weight.T,
                lengths,
                lambdas,
                head_gain[None],
            )
        )
    )
    got = lax.all_to_all(send.reshape(n_kv * n_tp, half, first), everyone, 0, 0, tiled=True)
    got = got.reshape(n_kv, n_tp, half, first)
    second = 2 * own_heads * VD + LANES
    rows = half * HEADS * 2
    send = pl.pallas_call(
        functools.partial(attend, width, piece),
        out_shape=jax.ShapeDtypeStruct((n_kv, n_tp, half, second), jnp.bfloat16),
        in_specs=[VMEM] * 6,
        out_specs=VMEM,
        compiler_params=PARAMS,
        scratch_shapes=[
            pltpu.VMEM((HEADS * half, LANES), jnp.float32),
            pltpu.VMEM((rows, LANES), jnp.float32),
            pltpu.VMEM((rows, LANES), jnp.float32),
        ],
    )(live, got, cache_keys, cache_values, pair_keys, pair_values)
    got = lax.all_to_all(send.reshape(n_kv * n_tp, half, second), everyone, 0, 0, tiled=True)
    partial_out, own = pl.pallas_call(
        functools.partial(finish, n_tp, piece),
        out_shape=(
            jax.ShapeDtypeStruct((seqs, output_weight.shape[1]), jnp.bfloat16),
            jax.ShapeDtypeStruct((seqs, LANES), jnp.float32),
        ),
        in_specs=[VMEM] * 3,
        out_specs=(VMEM, VMEM),
        compiler_params=PARAMS,
    )(tail, got, output_weight)
    new_keys = own[:, :k_cols].astype(jnp.bfloat16)
    new_values = own[:, k_cols : k_cols + v_cols].astype(jnp.bfloat16)
    out = partial_out.astype(jnp.float32)
    for step in range(1, n_tp):
        out = out + lax.ppermute(partial_out, "tp", [(i, i ^ step) for i in range(n_tp)]).astype(jnp.float32)
    return (out.astype(jnp.bfloat16), new_keys, new_values)


def solution(mesh):
    return jax.shard_map(
        body,
        mesh=mesh,
        in_specs=(
            P(None, "kv"),
            P("kv"),
            P("kv", "tp"),
            P("kv", "tp"),
            P("kv", "tp"),
            P(None, None, ("kv", "tp"), None),
            P(None, None, ("kv", "tp"), None),
            P(),
            P("tp"),
            P(),
            P("tp", "kv"),
        ),
        out_specs=(P(None, "kv"), P(None, "tp"), P(None, "tp")),
        check_vma=False,
    )
```

```python
import functools

import jax
import jax.numpy as jnp
from jax import lax
from jax.experimental import pallas as pl
from jax.experimental.pallas import tpu as pltpu
from jax.sharding import PartitionSpec as P

HEADS = 16
KV_HEADS = 2
QK = 64
VD = 128
LANES = 128
GROUP = HEADS // KV_HEADS
NEG_FILL = -1e30
VMEM = pl.BlockSpec(memory_space=pltpu.VMEM)
HBM = pl.BlockSpec(memory_space=pltpu.HBM)
PARAMS = pltpu.CompilerParams(vmem_limit_bytes=16 * 1024 * 1024)
CHUNKS = 2
SQUARES_AT = 96
OWN_AT = 64
CONTRACT_LAST = (((1,), (1,)), ((), ()))


def split3(x):
    high = x.astype(jnp.bfloat16).astype(jnp.float32)
    middle = (x - high).astype(jnp.bfloat16).astype(jnp.float32)
    low = x - high - middle
    return high, middle, low


def lane_of(shape):
    return lax.broadcasted_iota(jnp.int32, shape, 1)


def for_each(count, step):
    if count <= 8:
        for i in range(count):
            step(i)
    else:
        lax.fori_loop(0, count, lambda i, _: step(i), None)


def shifted(x, by):
    return pltpu.roll(x, lax.rem(by + 2 * LANES, LANES) if not isinstance(by, int) else by % LANES, 1)


def project(
    pos_count,
    tokens_hbm,
    gain_hbm,
    query_hbm,
    key_hbm,
    value_hbm,
    lengths_hbm,
    lambdas_hbm,
    head_gain_hbm,
    send_ref,
    left_ref,
    tail_ref,
    tokens_ref,
    gain_ref,
    query_ref,
    both_ref,
    lengths_ref,
    lambdas_ref,
    head_gain_ref,
    sems,
):
    n_kv, n_tp, half, _ = send_ref.shape
    seqs = tokens_hbm.shape[0]
    q_cols = query_hbm.shape[1]
    k_cols, v_cols = key_hbm.shape[0], value_hbm.shape[0]
    my_tp = lax.axis_index("tp")
    rows = query_hbm.shape[0] // CHUNKS
    chunks = [pl.ds(i * rows, rows) for i in range(CHUNKS)]
    pairs = [
        (tokens_hbm, tokens_ref),
        (gain_hbm, gain_ref),
        (key_hbm, both_ref.at[pl.ds(0, k_cols)]),
        (value_hbm, both_ref.at[pl.ds(k_cols, v_cols)]),
    ]
    pairs += [(query_hbm.at[chunk], query_ref.at[chunk]) for chunk in chunks]
    pairs += [(lengths_hbm, lengths_ref), (lambdas_hbm, lambdas_ref), (head_gain_hbm, head_gain_ref)]
    copies = [pltpu.make_async_copy(*pair, sems.at[i]) for i, pair in enumerate(pairs)]
    for copy in copies:
        copy.start()
    copies[0].wait()
    copies[1].wait()
    floats = tokens_ref[...].astype(jnp.float32)
    scaled = (floats * gain_ref[...]).astype(jnp.bfloat16)
    squares = jnp.sum(floats * floats, axis=1, keepdims=True)
    copies[2].wait()
    copies[3].wait()
    both = lax.dot_general(scaled, both_ref[...], CONTRACT_LAST, preferred_element_type=jnp.float32)
    if both.shape[1] < LANES:
        both = jnp.concatenate([both, jnp.zeros((seqs, LANES - both.shape[1]), jnp.float32)], axis=1)
    lane = lane_of((half, LANES))
    squares = jnp.where(lane == SQUARES_AT, squares[:half], squares[half:])
    piece = (k_cols + v_cols) // n_kv
    queries = jnp.zeros((seqs, q_cols), jnp.float32)
    for i in range(CHUNKS):
        copies[4 + i].wait()
        queries += jnp.dot(
            scaled[:, i * rows : (i + 1) * rows], query_ref[chunks[i], :], preferred_element_type=jnp.float32
        )

    def fill(v):
        slot = jnp.where(lane < 2 * piece, shifted(both[half:], piece - v * piece), squares)
        slot = jnp.where(lane < piece, shifted(both[:half], -v * piece), slot)
        for t in range(n_tp):
            send_ref[v, t, :, :q_cols] = queries[half:] if t % 2 else queries[:half]
            send_ref[v, t, :, q_cols:] = slot

    for_each(n_kv, fill)
    for copy in copies[4 + CHUNKS :]:
        copy.wait()
    core = lax.rem(my_tp, 2)
    own_block = lax.axis_index("kv") * n_tp + my_tp
    lane = lane_of((1, LANES))
    column_seq = lane // (2 * HEADS)
    for side, block in enumerate((own_block, own_block + 1 - 2 * core)):
        left = jnp.zeros((1, LANES), jnp.int32)
        for b in range(half):
            left = jnp.where(column_seq == b, lengths_ref[core * half + b] - block * pos_count, left)
        left_ref[side : side + 1, :] = left
    own_heads = lambdas_ref.shape[0]
    for g in range(own_heads):
        tail_ref[g : g + 1, :] = jnp.full((1, LANES), lambdas_ref[g], jnp.float32)
    tail_ref[own_heads : own_heads + 1, :] = head_gain_ref[...]


def attend(
    width,
    piece,
    left_ref,
    got_ref,
    keys_ref,
    values_ref,
    pair_keys_ref,
    pair_values_ref,
    send_ref,
    q_scr,
    o_scr,
):
    n_kv, n_tp, half, _ = send_ref.shape
    pos_count = keys_ref.shape[2]
    own_heads = HEADS // n_tp
    q_cols = own_heads * 2 * QK
    my_tp = lax.axis_index("tp")
    core = lax.rem(my_tp, 2)

    def add(v, sums):
        parts = [got_ref[v, t, :, :q_cols] for t in range(n_tp)] + [got_ref[v, my_tp, :, q_cols:]]
        return tuple(s + p for s, p in zip(sums, parts))

    zero = tuple(jnp.zeros((half, q_cols), jnp.float32) for _ in range(n_tp)) + (jnp.zeros((half, LANES), jnp.float32),)
    *totals, slot = lax.fori_loop(0, n_kv, add, zero, unroll=n_kv <= 8)
    inverses = [
        lax.rsqrt(slot[:, at : at + 1] / width + 1e-06) for at in (SQUARES_AT, SQUARES_AT + 1)
    ]
    inverse = jnp.where(core == 0, inverses[0], inverses[1])
    lane = lane_of((half, LANES))
    own = shifted(slot * jnp.where(lane < piece, inverses[0], inverses[1]), OWN_AT)
    per_seq = 2 * HEADS
    first_map = lane < QK
    for head in range(HEADS):
        t, g = divmod(head, own_heads)
        q = (totals[t][:, g * LANES : (g + 1) * LANES] * inverse).astype(jnp.bfloat16).astype(jnp.float32)
        q_scr[pl.ds(2 * head, half, stride=per_seq), :] = jnp.where(first_map, q, 0.0)
        q_scr[pl.ds(2 * head + 1, half, stride=per_seq), :] = jnp.where(first_map, 0.0, q)
    rows = 2 * GROUP
    pairs = [(b, h) for b in range(half) for h in range(KV_HEADS)]
    none = jnp.zeros((rows, LANES), jnp.bfloat16)
    queries = jnp.concatenate(
        [
            jnp.concatenate(
                [q_scr[i * rows : (i + 1) * rows, :].astype(jnp.bfloat16) if i == k else none for k in range(len(pairs))],
                axis=1,
            )
            for i in range(len(pairs))
        ],
        axis=0,
    )
    if queries.shape[0] < LANES:
        queries = jnp.concatenate(
            [queries, jnp.zeros((LANES - queries.shape[0], queries.shape[1]), jnp.bfloat16)], axis=0
        )
    row = lax.broadcasted_iota(jnp.int32, (pos_count, LANES), 0)
    lives, scores = [], []
    for side, ref in enumerate((keys_ref, pair_keys_ref)):
        keys = jnp.concatenate([ref[core * half + b, h] for b, h in pairs], axis=1)
        s = lax.dot_general(keys, queries, CONTRACT_LAST, preferred_element_type=jnp.float32) * QK ** (-0.5)
        live = row < left_ref[side : side + 1, :]
        lives.append(live)
        scores.append(jnp.where(live, s, NEG_FILL))
    peak = jnp.maximum(*(jnp.max(s, axis=0, keepdims=True) for s in scores))
    weights = [jnp.where(live, jnp.exp(s - peak), 0.0) for live, s in zip(lives, scores)]
    total = jnp.sum(weights[0], axis=0, keepdims=True) + jnp.sum(weights[1], axis=0, keepdims=True)
    some = total > 0.0
    total = jnp.where(some, total, 1.0)
    logs = jnp.where(some, peak + jnp.log(total), NEG_FILL)
    weights = (jnp.concatenate(weights, axis=0) * (1.0 / total)).T.astype(jnp.bfloat16)
    for i, (b, h) in enumerate(pairs):
        values = jnp.concatenate([ref[core * half + b, h] for ref in (values_ref, pair_values_ref)], axis=0)
        o_scr[i * rows : (i + 1) * rows, :] = jnp.dot(
            weights[i * rows : (i + 1) * rows], values, preferred_element_type=jnp.float32
        )
    per = 2 * own_heads
    logs = jnp.concatenate([shifted(logs, -b * per_seq) for b in range(half)], axis=0)
    parts = split3(logs)
    for t in range(n_tp):
        stats = own
        for k in reversed(range(3)):
            stats = jnp.where(lane < (k + 1) * per, shifted(parts[k], k * per - t * per), stats)
        stats = stats.astype(jnp.bfloat16)
        for j in range(per):
            o = o_scr[pl.ds(t * per + j, half, stride=per_seq), :].astype(jnp.bfloat16)
            for v in range(n_kv):
                send_ref[v, t, :, j * VD : (j + 1) * VD] = o
        for v in range(n_kv):
            send_ref[v, t, :, per * VD :] = stats


def finish(n_tp, piece, tail_ref, got_ref, weight_ref, out_ref, own_ref):
    count, half, _ = got_ref.shape
    own_heads = tail_ref.shape[0] - 1
    per = 2 * own_heads

    def logs_of(d):
        stats = got_ref[d, :, per * VD :].astype(jnp.float32)
        return stats + pltpu.roll(stats, LANES - per, 1) + pltpu.roll(stats, LANES - 2 * per, 1)

    lane = lane_of((half, LANES))
    for c in range(2):
        own_ref[c * half : (c + 1) * half, :] = jnp.zeros((half, LANES), jnp.float32)

    def collect(v):
        slot = got_ref[v * n_tp + lax.axis_index("tp"), :, per * VD :].astype(jnp.float32)
        inside = (lane >= v * piece) & (lane < (v + 1) * piece)
        for c in range(2):
            rows = slice(c * half, (c + 1) * half)
            own_ref[rows, :] = jnp.where(inside, shifted(slot, v * piece - OWN_AT - c * piece), own_ref[rows, :])

    for_each(count // n_tp, collect)
    parts = []
    for core in range(2):

        def peak_of(d, peak, core=core):
            return jnp.maximum(peak, logs_of(2 * d + core))

        def add(d, carry, core=core):
            total, *sums = carry
            share = jnp.exp(logs_of(2 * d + core) - peak)
            for j in range(per):
                got = got_ref[2 * d + core, :, j * VD : (j + 1) * VD].astype(jnp.float32)
                sums[j] = sums[j] + share[:, j : j + 1] * got
            return (total + share, *sums)

        unroll = count <= 32
        peak = lax.fori_loop(1, count // 2, peak_of, logs_of(core), unroll=unroll)
        zero = tuple(jnp.zeros((half, LANES), jnp.float32) for _ in range(per + 1))
        parts.append(lax.fori_loop(0, count // 2, add, zero, unroll=unroll))
    total, *sums = (jnp.concatenate(pair, axis=0) for pair in zip(*parts))
    inverse = 1.0 / total
    ratios = [sums[j] * inverse[:, j : j + 1] for j in range(per)]
    heads = []
    for g in range(own_heads):
        mixed = ratios[2 * g] - tail_ref[g : g + 1, :] * ratios[2 * g + 1]
        scale = lax.rsqrt(jnp.mean(mixed * mixed, axis=1, keepdims=True) + 1e-06)
        heads.append((mixed * scale * tail_ref[own_heads : own_heads + 1, :]).astype(jnp.bfloat16))
    flattened = jnp.concatenate(heads, axis=1)
    out_ref[...] = jnp.dot(flattened, weight_ref[...], preferred_element_type=jnp.float32).astype(jnp.bfloat16)


def body(
    tokens,
    norm_gain,
    query_weight,
    key_weight,
    value_weight,
    cache_keys,
    cache_values,
    lengths,
    lambdas,
    head_gain,
    output_weight,
):
    n_kv, n_tp = lax.axis_size("kv"), lax.axis_size("tp")
    everyone = ("kv", "tp")
    seqs = tokens.shape[0]
    half = seqs // 2
    own_heads = lambdas.shape[0]
    q_cols = query_weight.shape[1]
    k_cols, v_cols = key_weight.shape[1], value_weight.shape[1]
    pos_count = cache_keys.shape[2]
    width = tokens.shape[1] * n_kv
    cores = [(i, i ^ 1) for i in range(n_tp)]
    pair_keys = lax.ppermute(cache_keys, "tp", cores)
    pair_values = lax.ppermute(cache_values, "tp", cores)
    first = q_cols + LANES
    piece = (k_cols + v_cols) // n_kv
    send, left, tail = pl.pallas_call(
        functools.partial(project, pos_count),
        out_shape=(
            jax.ShapeDtypeStruct((n_kv, n_tp, half, first), jnp.float32),
            jax.ShapeDtypeStruct((2, LANES), jnp.int32),
            jax.ShapeDtypeStruct((own_heads + 1, LANES), jnp.float32),
        ),
        in_specs=[HBM] * 8,
        out_specs=(VMEM, VMEM, VMEM),
        scratch_shapes=[
            pltpu.VMEM(tokens.shape, tokens.dtype),
            pltpu.VMEM((1, tokens.shape[1]), jnp.float32),
            pltpu.VMEM(query_weight.shape, query_weight.dtype),
            pltpu.VMEM((k_cols + v_cols, tokens.shape[1]), key_weight.dtype),
            pltpu.SMEM(lengths.shape, lengths.dtype),
            pltpu.SMEM(lambdas.shape, lambdas.dtype),
            pltpu.VMEM((1, LANES), jnp.float32),
            pltpu.SemaphoreType.DMA((7 + CHUNKS,)),
        ],
        compiler_params=PARAMS,
    )(
        *(
            pltpu.with_memory_space_constraint(x, pltpu.HBM)
            for x in (
                tokens,
                norm_gain[None],
                query_weight,
                key_weight.T,
                value_weight.T,
                lengths,
                lambdas,
                head_gain[None],
            )
        )
    )
    got = lax.all_to_all(send.reshape(n_kv * n_tp, half, first), everyone, 0, 0, tiled=True)
    got = got.reshape(n_kv, n_tp, half, first)
    second = 2 * own_heads * VD + LANES
    rows = half * HEADS * 2
    send = pl.pallas_call(
        functools.partial(attend, width, piece),
        out_shape=jax.ShapeDtypeStruct((n_kv, n_tp, half, second), jnp.bfloat16),
        in_specs=[VMEM] * 6,
        out_specs=VMEM,
        compiler_params=PARAMS,
        scratch_shapes=[
            pltpu.VMEM((rows, LANES), jnp.float32),
            pltpu.VMEM((rows, LANES), jnp.float32),
        ],
    )(left, got, cache_keys, cache_values, pair_keys, pair_values)
    got = lax.all_to_all(send.reshape(n_kv * n_tp, half, second), everyone, 0, 0, tiled=True)
    partial_out, own = pl.pallas_call(
        functools.partial(finish, n_tp, piece),
        out_shape=(
            jax.ShapeDtypeStruct((seqs, output_weight.shape[1]), jnp.bfloat16),
            jax.ShapeDtypeStruct((seqs, LANES), jnp.float32),
        ),
        in_specs=[VMEM] * 3,
        out_specs=(VMEM, VMEM),
        compiler_params=PARAMS,
    )(tail, got, output_weight)
    new_keys = own[:, :k_cols].astype(jnp.bfloat16)
    new_values = own[:, k_cols : k_cols + v_cols].astype(jnp.bfloat16)
    out = partial_out.astype(jnp.float32)
    for step in range(1, n_tp):
        out = out + lax.ppermute(partial_out, "tp", [(i, i ^ step) for i in range(n_tp)]).astype(jnp.float32)
    return (out.astype(jnp.bfloat16), new_keys, new_values)


def solution(mesh):
    return jax.shard_map(
        body,
        mesh=mesh,
        in_specs=(
            P(None, "kv"),
            P("kv"),
            P("kv", "tp"),
            P("kv", "tp"),
            P("kv", "tp"),
            P(None, None, ("kv", "tp"), None),
            P(None, None, ("kv", "tp"), None),
            P(),
            P("tp"),
            P(),
            P("tp", "kv"),
        ),
        out_specs=(P(None, "kv"), P(None, "tp"), P(None, "tp")),
        check_vma=False,
    )
```

```python
import functools

import jax
import jax.numpy as jnp
from jax import lax
from jax.experimental import pallas as pl
from jax.experimental.pallas import tpu as pltpu
from jax.sharding import PartitionSpec as P

HEADS = 16
KV_HEADS = 2
QK = 64
VD = 128
LANES = 128
SUBLANES = 8
GROUP = HEADS // KV_HEADS
NEG_FILL = -1e30
VMEM = pl.BlockSpec(memory_space=pltpu.VMEM)
HBM = pl.BlockSpec(memory_space=pltpu.HBM)
PARAMS = pltpu.CompilerParams(vmem_limit_bytes=16 * 1024 * 1024)
CHUNKS = 2
SQUARES_AT = 96
OWN_AT = 64
CONTRACT_LAST = (((1,), (1,)), ((), ()))


def split3(x):
    high = x.astype(jnp.bfloat16).astype(jnp.float32)
    middle = (x - high).astype(jnp.bfloat16).astype(jnp.float32)
    low = x - high - middle
    return high, middle, low


def lane_of(shape):
    return lax.broadcasted_iota(jnp.int32, shape, 1)


def for_each(count, step):
    if count <= 32:
        for i in range(count):
            step(i)
    else:
        lax.fori_loop(0, count, lambda i, _: step(i), None)


def shifted(x, by):
    return pltpu.roll(x, lax.rem(by + 2 * LANES, LANES) if not isinstance(by, int) else by % LANES, 1)


def project(
    pos_count,
    tokens_hbm,
    gain_hbm,
    query_hbm,
    key_hbm,
    value_hbm,
    lengths_hbm,
    lambdas_hbm,
    head_gain_hbm,
    keys_hbm,
    values_hbm,
    send_ref,
    left_ref,
    tail_ref,
    give_ref,
    tokens_ref,
    gain_ref,
    query_ref,
    both_ref,
    lengths_ref,
    lambdas_ref,
    head_gain_ref,
    sems,
):
    n_kv, n_tp, half, _ = send_ref.shape
    seqs = tokens_hbm.shape[0]
    q_cols = query_hbm.shape[1]
    k_cols, v_cols = key_hbm.shape[0], value_hbm.shape[0]
    my_tp = lax.axis_index("tp")
    rows = query_hbm.shape[0] // CHUNKS
    chunks = [pl.ds(i * rows, rows) for i in range(CHUNKS)]
    pairs = [
        (tokens_hbm, tokens_ref),
        (gain_hbm, gain_ref),
        (key_hbm, both_ref.at[pl.ds(0, k_cols)]),
        (value_hbm, both_ref.at[pl.ds(k_cols, v_cols)]),
    ]
    pairs += [(query_hbm.at[chunk], query_ref.at[chunk]) for chunk in chunks]
    pairs += [(lengths_hbm, lengths_ref), (lambdas_hbm, lambdas_ref), (head_gain_hbm, head_gain_ref)]
    core = lax.rem(my_tp, 2)
    theirs = pl.ds((1 - core) * half, half)
    pairs += [(keys_hbm.at[theirs], give_ref.at[0]), (values_hbm.at[theirs], give_ref.at[1])]
    copies = [pltpu.make_async_copy(*pair, sems.at[i]) for i, pair in enumerate(pairs)]
    for copy in copies:
        copy.start()
    copies[0].wait()
    copies[1].wait()
    floats = tokens_ref[...].astype(jnp.float32)
    scaled = (floats * gain_ref[...]).astype(jnp.bfloat16)
    squares = jnp.sum(floats * floats, axis=1, keepdims=True)
    copies[2].wait()
    copies[3].wait()
    both = lax.dot_general(scaled, both_ref[...], CONTRACT_LAST, preferred_element_type=jnp.float32)
    if both.shape[1] < LANES:
        both = jnp.concatenate([both, jnp.zeros((seqs, LANES - both.shape[1]), jnp.float32)], axis=1)
    lane = lane_of((half, LANES))
    squares = jnp.where(lane == SQUARES_AT, squares[:half], squares[half:])
    piece = (k_cols + v_cols) // n_kv
    queries = jnp.zeros((seqs, q_cols), jnp.float32)
    for i in range(CHUNKS):
        copies[4 + i].wait()
        queries += jnp.dot(
            scaled[:, i * rows : (i + 1) * rows], query_ref[chunks[i], :], preferred_element_type=jnp.float32
        )

    def fill(v):
        slot = jnp.where(lane < 2 * piece, shifted(both[half:], piece - v * piece), squares)
        slot = jnp.where(lane < piece, shifted(both[:half], -v * piece), slot)
        for t in range(n_tp):
            send_ref[v, t, :, :q_cols] = queries[half:] if t % 2 else queries[:half]
            send_ref[v, t, :, q_cols:] = slot

    for_each(n_kv, fill)
    for copy in copies[4 + CHUNKS :]:
        copy.wait()
    own_block = lax.axis_index("kv") * n_tp + my_tp
    lane = lane_of((1, LANES))
    column_seq = lane // (2 * HEADS)
    for side, block in enumerate((own_block, own_block + 1 - 2 * core)):
        left = jnp.zeros((1, LANES), jnp.int32)
        for b in range(half):
            left = jnp.where(column_seq == b, lengths_ref[core * half + b] - block * pos_count, left)
        left_ref[side : side + 1, :] = left
    own_heads = lambdas_ref.shape[0]
    for g in range(own_heads):
        tail_ref[g : g + 1, :] = jnp.full((1, LANES), lambdas_ref[g], jnp.float32)
    tail_ref[own_heads : own_heads + 1, :] = head_gain_ref[...]


def attend(
    width,
    piece,
    left_ref,
    got_ref,
    keys_ref,
    values_ref,
    pair_ref,
    send_ref,
    q_scr,
    o_scr,
):
    n_kv, n_tp, half, _ = send_ref.shape
    pos_count = keys_ref.shape[2]
    own_heads = HEADS // n_tp
    q_cols = own_heads * 2 * QK
    my_tp = lax.axis_index("tp")
    core = lax.rem(my_tp, 2)

    def add(v, sums):
        parts = [got_ref[v, t, :, :q_cols] for t in range(n_tp)] + [got_ref[v, my_tp, :, q_cols:]]
        return tuple(s + p for s, p in zip(sums, parts))

    zero = tuple(jnp.zeros((half, q_cols), jnp.float32) for _ in range(n_tp)) + (jnp.zeros((half, LANES), jnp.float32),)
    *totals, slot = lax.fori_loop(0, n_kv, add, zero, unroll=n_kv <= 8)
    inverses = [
        lax.rsqrt(slot[:, at : at + 1] / width + 1e-06) for at in (SQUARES_AT, SQUARES_AT + 1)
    ]
    inverse = jnp.where(core == 0, inverses[0], inverses[1])
    lane = lane_of((half, LANES))
    own = shifted(slot * jnp.where(lane < piece, inverses[0], inverses[1]), OWN_AT)
    per_seq = 2 * HEADS
    first_map = lane < QK
    for head in range(HEADS):
        t, g = divmod(head, own_heads)
        q = (totals[t][:, g * LANES : (g + 1) * LANES] * inverse).astype(jnp.bfloat16).astype(jnp.float32)
        q_scr[pl.ds(2 * head, half, stride=per_seq), :] = jnp.where(first_map, q, 0.0)
        q_scr[pl.ds(2 * head + 1, half, stride=per_seq), :] = jnp.where(first_map, 0.0, q)
    rows = 2 * GROUP
    pairs = [(b, h) for b in range(half) for h in range(KV_HEADS)]
    none = jnp.zeros((rows, LANES), jnp.bfloat16)
    queries = jnp.concatenate(
        [
            jnp.concatenate(
                [q_scr[i * rows : (i + 1) * rows, :].astype(jnp.bfloat16) if i == k else none for k in range(len(pairs))],
                axis=1,
            )
            for i in range(len(pairs))
        ],
        axis=0,
    )
    if queries.shape[0] < LANES:
        queries = jnp.concatenate(
            [queries, jnp.zeros((LANES - queries.shape[0], queries.shape[1]), jnp.bfloat16)], axis=0
        )
    row = lax.broadcasted_iota(jnp.int32, (pos_count, LANES), 0)
    lives, scores = [], []
    for side in range(2):
        blocks = [pair_ref[0, b, h] if side else keys_ref[core * half + b, h] for b, h in pairs]
        keys = jnp.concatenate(blocks, axis=1)
        s = lax.dot_general(keys, queries, CONTRACT_LAST, preferred_element_type=jnp.float32) * QK ** (-0.5)
        live = row < left_ref[side : side + 1, :]
        lives.append(live)
        scores.append(jnp.where(live, s, NEG_FILL))
    peak = jnp.maximum(*(jnp.max(s, axis=0, keepdims=True) for s in scores))
    weights = [jnp.where(live, jnp.exp(s - peak), 0.0) for live, s in zip(lives, scores)]
    total = jnp.sum(weights[0], axis=0, keepdims=True) + jnp.sum(weights[1], axis=0, keepdims=True)
    some = total > 0.0
    total = jnp.where(some, total, 1.0)
    logs = jnp.where(some, peak + jnp.log(total), NEG_FILL)
    weights = (jnp.concatenate(weights, axis=0) * (1.0 / total)).T.astype(jnp.bfloat16)
    for i, (b, h) in enumerate(pairs):
        values = jnp.concatenate([values_ref[core * half + b, h], pair_ref[1, b, h]], axis=0)
        o_scr[i * rows : (i + 1) * rows, :] = jnp.dot(
            weights[i * rows : (i + 1) * rows], values, preferred_element_type=jnp.float32
        )
    per = 2 * own_heads
    logs = jnp.concatenate([shifted(logs, -b * per_seq) for b in range(half)], axis=0)
    parts = split3(logs)
    for t in range(n_tp):
        stats = own
        for k in reversed(range(3)):
            stats = jnp.where(lane < (k + 1) * per, shifted(parts[k], k * per - t * per), stats)
        stats = stats.astype(jnp.bfloat16)
        for j in range(per):
            o = o_scr[pl.ds(t * per + j, half, stride=per_seq), :].astype(jnp.bfloat16)
            for v in range(n_kv):
                send_ref[v, t, :, j * VD : (j + 1) * VD] = o
        for v in range(n_kv):
            send_ref[v, t, :, per * VD :] = stats


def finish(n_tp, piece, tail_ref, got_ref, weight_ref, out_ref, own_ref, log_scr, share_scr):
    count, half, _ = got_ref.shape
    own_heads = tail_ref.shape[0] - 1
    per = 2 * own_heads
    rows = count * half
    my_tp = lax.axis_index("tp")
    unroll = count <= 32

    def stage(d):
        log_scr[pl.ds(d * half, half), :] = got_ref[d, :, per * VD :].astype(jnp.float32)

    for_each(count, stage)
    logs = log_scr[...]
    logs = logs + shifted(logs, -per) + shifted(logs, -2 * per)
    logs = logs.reshape(rows // SUBLANES, SUBLANES, LANES)

    def over_sources(x, combine):
        by = 2 * half
        while by < SUBLANES:
            x = combine(x, pltpu.roll(x, by, 0))
            by *= 2
        return x

    peak = over_sources(jnp.max(logs, axis=0), jnp.maximum)
    shares = jnp.exp(logs - peak[None])
    shares = shares * (1.0 / over_sources(jnp.sum(shares, axis=0), jnp.add))[None]
    shares = shares.reshape(rows, LANES)
    for j in range(per):
        share_scr[j] = jnp.broadcast_to(shares[:, j : j + 1], (rows, LANES))
    ratios = []
    for j in range(per):

        def add(i, sums, j=j):
            return tuple(
                x
                + share_scr[j, pl.ds((2 * i + c) * half, half), :]
                * got_ref[2 * i + c, :, j * VD : (j + 1) * VD].astype(jnp.float32)
                for c, x in enumerate(sums)
            )

        zero = jnp.zeros((half, VD), jnp.float32)
        ratios.append(jnp.concatenate(lax.fori_loop(0, count // 2, add, (zero, zero), unroll=unroll), axis=0))
    heads = []
    for g in range(own_heads):
        mixed = ratios[2 * g] - tail_ref[g : g + 1, :] * ratios[2 * g + 1]
        scale = lax.rsqrt(jnp.mean(mixed * mixed, axis=1, keepdims=True) + 1e-06)
        heads.append((mixed * scale * tail_ref[own_heads : own_heads + 1, :]).astype(jnp.bfloat16))
    flattened = jnp.concatenate(heads, axis=1)
    out_ref[...] = jnp.dot(flattened, weight_ref[...], preferred_element_type=jnp.float32).astype(jnp.bfloat16)
    lane = lane_of((half, LANES))

    def collect(v, own):
        slot = log_scr[pl.ds((v * n_tp + my_tp) * half, half), :]
        inside = (lane >= v * piece) & (lane < (v + 1) * piece)
        return tuple(
            jnp.where(inside, shifted(slot, v * piece - OWN_AT - c * piece), x) for c, x in enumerate(own)
        )

    zero = jnp.zeros((half, LANES), jnp.float32)
    own = lax.fori_loop(0, count // n_tp, collect, (zero, zero), unroll=count // n_tp <= 8)
    own_ref[...] = jnp.concatenate(own, axis=0)


def body(
    tokens,
    norm_gain,
    query_weight,
    key_weight,
    value_weight,
    cache_keys,
    cache_values,
    lengths,
    lambdas,
    head_gain,
    output_weight,
):
    n_kv, n_tp = lax.axis_size("kv"), lax.axis_size("tp")
    everyone = ("kv", "tp")
    seqs = tokens.shape[0]
    half = seqs // 2
    own_heads = lambdas.shape[0]
    q_cols = query_weight.shape[1]
    k_cols, v_cols = key_weight.shape[1], value_weight.shape[1]
    pos_count = cache_keys.shape[2]
    width = tokens.shape[1] * n_kv
    first = q_cols + LANES
    piece = (k_cols + v_cols) // n_kv
    send, left, tail, give = pl.pallas_call(
        functools.partial(project, pos_count),
        out_shape=(
            jax.ShapeDtypeStruct((n_kv, n_tp, half, first), jnp.float32),
            jax.ShapeDtypeStruct((2, LANES), jnp.int32),
            jax.ShapeDtypeStruct((own_heads + 1, LANES), jnp.float32),
            jax.ShapeDtypeStruct((2, half, *cache_keys.shape[1:]), cache_keys.dtype),
        ),
        in_specs=[HBM] * 10,
        out_specs=(VMEM,) * 4,
        scratch_shapes=[
            pltpu.VMEM(tokens.shape, tokens.dtype),
            pltpu.VMEM((1, tokens.shape[1]), jnp.float32),
            pltpu.VMEM(query_weight.shape, query_weight.dtype),
            pltpu.VMEM((k_cols + v_cols, tokens.shape[1]), key_weight.dtype),
            pltpu.SMEM(lengths.shape, lengths.dtype),
            pltpu.SMEM(lambdas.shape, lambdas.dtype),
            pltpu.VMEM((1, LANES), jnp.float32),
            pltpu.SemaphoreType.DMA((9 + CHUNKS,)),
        ],
        compiler_params=PARAMS,
    )(
        *(
            pltpu.with_memory_space_constraint(x, pltpu.HBM)
            for x in (
                tokens,
                norm_gain[None],
                query_weight,
                key_weight.T,
                value_weight.T,
                lengths,
                lambdas,
                head_gain[None],
                cache_keys,
                cache_values,
            )
        )
    )
    pair = lax.ppermute(give, "tp", [(i, i ^ 1) for i in range(n_tp)])
    got = lax.all_to_all(send.reshape(n_kv * n_tp, half, first), everyone, 0, 0, tiled=True)
    got = got.reshape(n_kv, n_tp, half, first)
    second = 2 * own_heads * VD + LANES
    rows = half * HEADS * 2
    send = pl.pallas_call(
        functools.partial(attend, width, piece),
        out_shape=jax.ShapeDtypeStruct((n_kv, n_tp, half, second), jnp.bfloat16),
        in_specs=[VMEM] * 5,
        out_specs=VMEM,
        compiler_params=PARAMS,
        scratch_shapes=[
            pltpu.VMEM((rows, LANES), jnp.float32),
            pltpu.VMEM((rows, LANES), jnp.float32),
        ],
    )(left, got, cache_keys, cache_values, pair)
    got = lax.all_to_all(send.reshape(n_kv * n_tp, half, second), everyone, 0, 0, tiled=True)
    partial_out, own = pl.pallas_call(
        functools.partial(finish, n_tp, piece),
        out_shape=(
            jax.ShapeDtypeStruct((seqs, output_weight.shape[1]), jnp.bfloat16),
            jax.ShapeDtypeStruct((seqs, LANES), jnp.float32),
        ),
        in_specs=[VMEM] * 3,
        out_specs=(VMEM, VMEM),
        compiler_params=PARAMS,
        scratch_shapes=[
            pltpu.VMEM((n_kv * n_tp * half, LANES), jnp.float32),
            pltpu.VMEM((2 * own_heads, n_kv * n_tp * half, LANES), jnp.float32),
        ],
    )(tail, got, output_weight)
    new_keys = own[:, :k_cols].astype(jnp.bfloat16)
    new_values = own[:, k_cols : k_cols + v_cols].astype(jnp.bfloat16)
    out = partial_out.astype(jnp.float32)
    for step in range(1, n_tp):
        out = out + lax.ppermute(partial_out, "tp", [(i, i ^ step) for i in range(n_tp)]).astype(jnp.float32)
    return (out.astype(jnp.bfloat16), new_keys, new_values)


def solution(mesh):
    return jax.shard_map(
        body,
        mesh=mesh,
        in_specs=(
            P(None, "kv"),
            P("kv"),
            P("kv", "tp"),
            P("kv", "tp"),
            P("kv", "tp"),
            P(None, None, ("kv", "tp"), None),
            P(None, None, ("kv", "tp"), None),
            P(),
            P("tp"),
            P(),
            P("tp", "kv"),
        ),
        out_specs=(P(None, "kv"), P(None, "tp"), P(None, "tp")),
        check_vma=False,
    )
```

```python
import functools

import jax
import jax.numpy as jnp
from jax import lax
from jax.experimental import pallas as pl
from jax.experimental.pallas import tpu as pltpu
from jax.sharding import PartitionSpec as P

HEADS = 16
KV_HEADS = 2
QK = 64
VD = 128
LANES = 128
SUBLANES = 8
GROUP = HEADS // KV_HEADS
NEG_FILL = -1e30
VMEM = pl.BlockSpec(memory_space=pltpu.VMEM)
HBM = pl.BlockSpec(memory_space=pltpu.HBM)
PARAMS = pltpu.CompilerParams(vmem_limit_bytes=16 * 1024 * 1024)
CHUNKS = 2
SQUARES_AT = 96
OWN_AT = 64
CONTRACT_LAST = (((1,), (1,)), ((), ()))


def split3(x):
    high = x.astype(jnp.bfloat16).astype(jnp.float32)
    middle = (x - high).astype(jnp.bfloat16).astype(jnp.float32)
    low = x - high - middle
    return high, middle, low


def lane_of(shape):
    return lax.broadcasted_iota(jnp.int32, shape, 1)


def for_each(count, step):
    if count <= 32:
        for i in range(count):
            step(i)
    else:
        lax.fori_loop(0, count, lambda i, _: step(i), None)


def shifted(x, by):
    return pltpu.roll(x, lax.rem(by + 2 * LANES, LANES) if not isinstance(by, int) else by % LANES, 1)


def project(
    pos_count,
    tokens_hbm,
    gain_hbm,
    query_hbm,
    key_hbm,
    value_hbm,
    lengths_hbm,
    lambdas_hbm,
    head_gain_hbm,
    keys_hbm,
    values_hbm,
    send_ref,
    left_ref,
    tail_ref,
    give_ref,
    have_ref,
    tokens_ref,
    gain_ref,
    query_ref,
    both_ref,
    lengths_ref,
    lambdas_ref,
    head_gain_ref,
    row_scr,
    sems,
):
    n_kv, n_tp = send_ref.shape[:2]
    seqs = tokens_hbm.shape[0]
    half = seqs // 2
    q_cols = query_hbm.shape[1]
    k_cols, v_cols = key_hbm.shape[0], value_hbm.shape[0]
    my_tp = lax.axis_index("tp")
    rows = query_hbm.shape[0] // CHUNKS
    chunks = [pl.ds(i * rows, rows) for i in range(CHUNKS)]
    pairs = [
        (tokens_hbm, tokens_ref),
        (gain_hbm, gain_ref),
        (key_hbm, both_ref.at[pl.ds(0, k_cols)]),
        (value_hbm, both_ref.at[pl.ds(k_cols, v_cols)]),
    ]
    pairs += [(query_hbm.at[chunk], query_ref.at[chunk]) for chunk in chunks]
    pairs += [(lengths_hbm, lengths_ref), (lambdas_hbm, lambdas_ref), (head_gain_hbm, head_gain_ref)]
    core = lax.rem(my_tp, 2)
    for taker, block_ref in ((1 - core, give_ref), (core, have_ref)):
        of_taker = pl.ds(taker * half, half)
        pairs += [(keys_hbm.at[of_taker], block_ref.at[0]), (values_hbm.at[of_taker], block_ref.at[1])]
    copies = [pltpu.make_async_copy(*pair, sems.at[i]) for i, pair in enumerate(pairs)]
    for copy in copies:
        copy.start()
    copies[0].wait()
    copies[1].wait()
    floats = tokens_ref[...].astype(jnp.float32)
    scaled = (floats * gain_ref[...]).astype(jnp.bfloat16)
    squares = jnp.sum(floats * floats, axis=1, keepdims=True)
    copies[2].wait()
    copies[3].wait()
    both = lax.dot_general(scaled, both_ref[...], CONTRACT_LAST, preferred_element_type=jnp.float32)
    if both.shape[1] < LANES:
        both = jnp.concatenate([both, jnp.zeros((seqs, LANES - both.shape[1]), jnp.float32)], axis=1)
    piece = (k_cols + v_cols) // n_kv
    both = jnp.concatenate([shifted(both[i : i + 1], i * piece) for i in range(seqs)], axis=0)
    lane = lane_of((seqs, LANES))
    row = lax.broadcasted_iota(jnp.int32, (seqs, LANES), 0)
    squares = jnp.where(lane == SQUARES_AT + row, squares, 0.0)
    queries = jnp.zeros((seqs, q_cols), jnp.float32)
    for i in range(CHUNKS):
        copies[4 + i].wait()
        queries += jnp.dot(
            scaled[:, i * rows : (i + 1) * rows], query_ref[chunks[i], :], preferred_element_type=jnp.float32
        )

    for i in range(seqs):
        row_scr[i // half, :, i % half * q_cols : (i % half + 1) * q_cols] = queries[i : i + 1]
    queries = [row_scr[c] for c in range(2)]

    def fill(v):
        slot = jnp.where(lane // piece == row, shifted(both, -v * piece), squares)
        slot = jnp.sum(slot, axis=0, keepdims=True)
        for t in range(n_tp):
            send_ref[v, t, :, : half * q_cols] = queries[t % 2]
            send_ref[v, t, :, half * q_cols :] = slot

    for_each(n_kv, fill)
    for copy in copies[4 + CHUNKS :]:
        copy.wait()
    own_block = lax.axis_index("kv") * n_tp + my_tp
    lane = lane_of((1, LANES))
    column_seq = lane // (2 * HEADS)
    for side, block in enumerate((own_block, own_block + 1 - 2 * core)):
        left = jnp.zeros((1, LANES), jnp.int32)
        for b in range(half):
            left = jnp.where(column_seq == b, lengths_ref[core * half + b] - block * pos_count, left)
        left_ref[side : side + 1, :] = left
    own_heads = lambdas_ref.shape[0]
    for g in range(own_heads):
        tail_ref[g : g + 1, :] = jnp.full((1, LANES), lambdas_ref[g], jnp.float32)
    tail_ref[own_heads : own_heads + 1, :] = head_gain_ref[...]


def attend(
    width,
    piece,
    left_ref,
    got_ref,
    have_ref,
    pair_ref,
    send_ref,
    q_scr,
    o_scr,
):
    n_kv, n_tp, half, _ = send_ref.shape
    pos_count = have_ref.shape[3]
    own_heads = HEADS // n_tp
    q_cols = own_heads * 2 * QK
    my_tp = lax.axis_index("tp")
    core = lax.rem(my_tp, 2)

    def add(v, sums):
        parts = [got_ref[v, t, :, : half * q_cols] for t in range(n_tp)] + [got_ref[v, my_tp, :, half * q_cols :]]
        return tuple(s + p for s, p in zip(sums, parts))

    zero = tuple(jnp.zeros((1, half * q_cols), jnp.float32) for _ in range(n_tp)) + (jnp.zeros((1, LANES), jnp.float32),)
    *totals, slot = lax.fori_loop(0, n_kv, add, zero, unroll=n_kv <= 8)
    inverses = [
        lax.rsqrt(slot[:, at : at + 1] / width + 1e-06) for at in range(SQUARES_AT, SQUARES_AT + 2 * half)
    ]
    lane = lane_of((1, LANES))
    scale = jnp.zeros((1, LANES), jnp.float32)
    for i, inverse in enumerate(inverses):
        scale = jnp.where(lane // piece == i, inverse, scale)
    own = jnp.concatenate([shifted(slot * scale, OWN_AT), jnp.zeros((half - 1, LANES), jnp.float32)], axis=0)
    per_seq = 2 * HEADS
    first_map = lane_of((1, q_cols)) % LANES < QK
    for b in range(half):
        inverse = jnp.where(core == 0, inverses[b], inverses[half + b])
        for t in range(n_tp):
            q = (totals[t][:, b * q_cols : (b + 1) * q_cols] * inverse).astype(jnp.bfloat16).astype(jnp.float32)
            maps = jnp.where(first_map, q, 0.0), jnp.where(first_map, 0.0, q)
            for g in range(own_heads):
                at = b * per_seq + 2 * (t * own_heads + g)
                for c in range(2):
                    q_scr[at + c : at + c + 1, :] = maps[c][:, g * LANES : (g + 1) * LANES]
    lane = lane_of((half, LANES))
    rows = 2 * GROUP
    pairs = [(b, h) for b in range(half) for h in range(KV_HEADS)]
    none = jnp.zeros((rows, LANES), jnp.bfloat16)
    queries = jnp.concatenate(
        [
            jnp.concatenate(
                [q_scr[i * rows : (i + 1) * rows, :].astype(jnp.bfloat16) if i == k else none for k in range(len(pairs))],
                axis=1,
            )
            for i in range(len(pairs))
        ],
        axis=0,
    )
    if queries.shape[0] < LANES:
        queries = jnp.concatenate(
            [queries, jnp.zeros((LANES - queries.shape[0], queries.shape[1]), jnp.bfloat16)], axis=0
        )
    row = lax.broadcasted_iota(jnp.int32, (pos_count, LANES), 0)
    lives, scores = [], []
    for side in range(2):
        blocks = [(have_ref, pair_ref)[side][0, b, h] for b, h in pairs]
        keys = jnp.concatenate(blocks, axis=1)
        s = lax.dot_general(keys, queries, CONTRACT_LAST, preferred_element_type=jnp.float32) * QK ** (-0.5)
        live = row < left_ref[side : side + 1, :]
        lives.append(live)
        scores.append(jnp.where(live, s, NEG_FILL))
    peak = jnp.maximum(*(jnp.max(s, axis=0, keepdims=True) for s in scores))
    weights = [jnp.where(live, jnp.exp(s - peak), 0.0) for live, s in zip(lives, scores)]
    total = jnp.sum(weights[0], axis=0, keepdims=True) + jnp.sum(weights[1], axis=0, keepdims=True)
    some = total > 0.0
    total = jnp.where(some, total, 1.0)
    logs = jnp.where(some, peak + jnp.log(total), NEG_FILL)
    weights = (jnp.concatenate(weights, axis=0) * (1.0 / total)).T.astype(jnp.bfloat16)
    for i, (b, h) in enumerate(pairs):
        values = jnp.concatenate([have_ref[1, b, h], pair_ref[1, b, h]], axis=0)
        o_scr[i * rows : (i + 1) * rows, :] = jnp.dot(
            weights[i * rows : (i + 1) * rows], values, preferred_element_type=jnp.float32
        )
    per = 2 * own_heads
    logs = jnp.concatenate([shifted(logs, -b * per_seq) for b in range(half)], axis=0)
    parts = split3(logs)
    for t in range(n_tp):
        stats = own
        for k in reversed(range(3)):
            stats = jnp.where(lane < (k + 1) * per, shifted(parts[k], k * per - t * per), stats)
        stats = stats.astype(jnp.bfloat16)
        for j in range(per):
            o = o_scr[pl.ds(t * per + j, half, stride=per_seq), :].astype(jnp.bfloat16)
            for v in range(n_kv):
                send_ref[v, t, :, j * VD : (j + 1) * VD] = o
        for v in range(n_kv):
            send_ref[v, t, :, per * VD :] = stats


def finish(n_tp, piece, tail_ref, got_ref, weight_ref, out_ref, own_ref, log_scr, share_scr):
    count, half, _ = got_ref.shape
    own_heads = tail_ref.shape[0] - 1
    per = 2 * own_heads
    rows = count * half
    my_tp = lax.axis_index("tp")
    unroll = count <= 32

    def stage(d):
        log_scr[pl.ds(d * half, half), :] = got_ref[d, :, per * VD :].astype(jnp.float32)

    for_each(count, stage)
    logs = log_scr[...]
    logs = logs + shifted(logs, -per) + shifted(logs, -2 * per)
    logs = logs.reshape(rows // SUBLANES, SUBLANES, LANES)

    def over_sources(x, combine):
        by = 2 * half
        while by < SUBLANES:
            x = combine(x, pltpu.roll(x, by, 0))
            by *= 2
        return x

    peak = over_sources(jnp.max(logs, axis=0), jnp.maximum)
    shares = jnp.exp(logs - peak[None])
    shares = shares * (1.0 / over_sources(jnp.sum(shares, axis=0), jnp.add))[None]
    shares = shares.reshape(rows, LANES)
    for j in range(per):
        share_scr[j] = jnp.broadcast_to(shares[:, j : j + 1], (rows, LANES))
    ratios = []
    for j in range(per):

        def add(i, sums, j=j):
            return tuple(
                x
                + share_scr[j, pl.ds((2 * i + c) * half, half), :]
                * got_ref[2 * i + c, :, j * VD : (j + 1) * VD].astype(jnp.float32)
                for c, x in enumerate(sums)
            )

        zero = jnp.zeros((half, VD), jnp.float32)
        ratios.append(jnp.concatenate(lax.fori_loop(0, count // 2, add, (zero, zero), unroll=unroll), axis=0))
    heads = []
    for g in range(own_heads):
        mixed = ratios[2 * g] - tail_ref[g : g + 1, :] * ratios[2 * g + 1]
        scale = lax.rsqrt(jnp.mean(mixed * mixed, axis=1, keepdims=True) + 1e-06)
        heads.append((mixed * scale * tail_ref[own_heads : own_heads + 1, :]).astype(jnp.bfloat16))
    flattened = jnp.concatenate(heads, axis=1)
    out_ref[...] = jnp.dot(flattened, weight_ref[...], preferred_element_type=jnp.float32).astype(jnp.bfloat16)
    lane = lane_of((1, LANES))

    def collect(v, own):
        slot = log_scr[pl.ds((v * n_tp + my_tp) * half, 1), :]
        inside = (lane >= v * piece) & (lane < (v + 1) * piece)
        return tuple(
            jnp.where(inside, shifted(slot, v * piece - OWN_AT - i * piece), x) for i, x in enumerate(own)
        )

    zero = (jnp.zeros((1, LANES), jnp.float32),) * (2 * half)
    own = lax.fori_loop(0, count // n_tp, collect, zero, unroll=count // n_tp <= 8)
    own_ref[...] = jnp.concatenate(own, axis=0)


def body(
    tokens,
    norm_gain,
    query_weight,
    key_weight,
    value_weight,
    cache_keys,
    cache_values,
    lengths,
    lambdas,
    head_gain,
    output_weight,
):
    n_kv, n_tp = lax.axis_size("kv"), lax.axis_size("tp")
    everyone = ("kv", "tp")
    seqs = tokens.shape[0]
    half = seqs // 2
    own_heads = lambdas.shape[0]
    q_cols = query_weight.shape[1]
    k_cols, v_cols = key_weight.shape[1], value_weight.shape[1]
    pos_count = cache_keys.shape[2]
    width = tokens.shape[1] * n_kv
    first = half * q_cols + LANES
    piece = (k_cols + v_cols) // n_kv
    send, left, tail, give, have = pl.pallas_call(
        functools.partial(project, pos_count),
        out_shape=(
            jax.ShapeDtypeStruct((n_kv, n_tp, 1, first), jnp.float32),
            jax.ShapeDtypeStruct((2, LANES), jnp.int32),
            jax.ShapeDtypeStruct((own_heads + 1, LANES), jnp.float32),
            jax.ShapeDtypeStruct((2, half, *cache_keys.shape[1:]), cache_keys.dtype),
            jax.ShapeDtypeStruct((2, half, *cache_keys.shape[1:]), cache_keys.dtype),
        ),
        in_specs=[HBM] * 10,
        out_specs=(VMEM,) * 5,
        scratch_shapes=[
            pltpu.VMEM(tokens.shape, tokens.dtype),
            pltpu.VMEM((1, tokens.shape[1]), jnp.float32),
            pltpu.VMEM(query_weight.shape, query_weight.dtype),
            pltpu.VMEM((k_cols + v_cols, tokens.shape[1]), key_weight.dtype),
            pltpu.SMEM(lengths.shape, lengths.dtype),
            pltpu.SMEM(lambdas.shape, lambdas.dtype),
            pltpu.VMEM((1, LANES), jnp.float32),
            pltpu.VMEM((2, 1, half * q_cols), jnp.float32),
            pltpu.SemaphoreType.DMA((11 + CHUNKS,)),
        ],
        compiler_params=PARAMS,
    )(
        *(
            pltpu.with_memory_space_constraint(x, pltpu.HBM)
            for x in (
                tokens,
                norm_gain[None],
                query_weight,
                key_weight.T,
                value_weight.T,
                lengths,
                lambdas,
                head_gain[None],
                cache_keys,
                cache_values,
            )
        )
    )
    pair = lax.ppermute(give, "tp", [(i, i ^ 1) for i in range(n_tp)])
    got = lax.all_to_all(send.reshape(n_kv * n_tp, 1, first), everyone, 0, 0, tiled=True)
    got = got.reshape(n_kv, n_tp, 1, first)
    second = 2 * own_heads * VD + LANES
    rows = half * HEADS * 2
    send = pl.pallas_call(
        functools.partial(attend, width, piece),
        out_shape=jax.ShapeDtypeStruct((n_kv, n_tp, half, second), jnp.bfloat16),
        in_specs=[VMEM] * 4,
        out_specs=VMEM,
        compiler_params=PARAMS,
        scratch_shapes=[
            pltpu.VMEM((rows, LANES), jnp.float32),
            pltpu.VMEM((rows, LANES), jnp.float32),
        ],
    )(left, got, have, pair)
    got = lax.all_to_all(send.reshape(n_kv * n_tp, half, second), everyone, 0, 0, tiled=True)
    partial_out, own = pl.pallas_call(
        functools.partial(finish, n_tp, piece),
        out_shape=(
            jax.ShapeDtypeStruct((seqs, output_weight.shape[1]), jnp.bfloat16),
            jax.ShapeDtypeStruct((seqs, LANES), jnp.float32),
        ),
        in_specs=[VMEM] * 3,
        out_specs=(VMEM, VMEM),
        compiler_params=PARAMS,
        scratch_shapes=[
            pltpu.VMEM((n_kv * n_tp * half, LANES), jnp.float32),
            pltpu.VMEM((2 * own_heads, n_kv * n_tp * half, LANES), jnp.float32),
        ],
    )(tail, got, output_weight)
    new_keys = own[:, :k_cols].astype(jnp.bfloat16)
    new_values = own[:, k_cols : k_cols + v_cols].astype(jnp.bfloat16)
    out = partial_out.astype(jnp.float32)
    for step in range(1, n_tp):
        out = out + lax.ppermute(partial_out, "tp", [(i, i ^ step) for i in range(n_tp)]).astype(jnp.float32)
    return (out.astype(jnp.bfloat16), new_keys, new_values)


def solution(mesh):
    return jax.shard_map(
        body,
        mesh=mesh,
        in_specs=(
            P(None, "kv"),
            P("kv"),
            P("kv", "tp"),
            P("kv", "tp"),
            P("kv", "tp"),
            P(None, None, ("kv", "tp"), None),
            P(None, None, ("kv", "tp"), None),
            P(),
            P("tp"),
            P(),
            P("tp", "kv"),
        ),
        out_specs=(P(None, "kv"), P(None, "tp"), P(None, "tp")),
        check_vma=False,
    )
```

```python
import functools

import jax
import jax.numpy as jnp
from jax import lax
from jax.experimental import pallas as pl
from jax.experimental.pallas import tpu as pltpu
from jax.sharding import PartitionSpec as P

HEADS = 16
KV_HEADS = 2
QK = 64
VD = 128
LANES = 128
SUBLANES = 8
GROUP = HEADS // KV_HEADS
NEG_FILL = -1e30
VMEM = pl.BlockSpec(memory_space=pltpu.VMEM)
HBM = pl.BlockSpec(memory_space=pltpu.HBM)
PARAMS = pltpu.CompilerParams(vmem_limit_bytes=16 * 1024 * 1024)
CHUNKS = 2
SQUARES_AT = 96
OWN_AT = 64
CONTRACT_LAST = (((1,), (1,)), ((), ()))


def split3(x):
    high = x.astype(jnp.bfloat16).astype(jnp.float32)
    middle = (x - high).astype(jnp.bfloat16).astype(jnp.float32)
    low = x - high - middle
    return high, middle, low


def lane_of(shape):
    return lax.broadcasted_iota(jnp.int32, shape, 1)


def for_each(count, step):
    if count <= 32:
        for i in range(count):
            step(i)
    else:
        lax.fori_loop(0, count, lambda i, _: step(i), None)


def shifted(x, by):
    return pltpu.roll(x, lax.rem(by + 2 * LANES, LANES) if not isinstance(by, int) else by % LANES, 1)


def project(
    pos_count,
    tokens_hbm,
    gain_hbm,
    query_hbm,
    key_hbm,
    value_hbm,
    lengths_hbm,
    lambdas_hbm,
    head_gain_hbm,
    keys_hbm,
    values_hbm,
    send_ref,
    left_ref,
    tail_ref,
    give_ref,
    have_ref,
    tokens_ref,
    gain_ref,
    query_ref,
    both_ref,
    lengths_ref,
    lambdas_ref,
    head_gain_ref,
    row_scr,
    sems,
):
    n_kv, n_tp = send_ref.shape[:2]
    seqs = tokens_hbm.shape[0]
    half = seqs // 2
    q_cols = query_hbm.shape[1]
    k_cols, v_cols = key_hbm.shape[0], value_hbm.shape[0]
    my_tp = lax.axis_index("tp")
    rows = query_hbm.shape[0] // CHUNKS
    chunks = [pl.ds(i * rows, rows) for i in range(CHUNKS)]
    pairs = [
        (tokens_hbm, tokens_ref),
        (gain_hbm, gain_ref),
        (key_hbm, both_ref.at[pl.ds(0, k_cols)]),
        (value_hbm, both_ref.at[pl.ds(k_cols, v_cols)]),
    ]
    pairs += [(query_hbm.at[chunk], query_ref.at[chunk]) for chunk in chunks]
    pairs += [(lengths_hbm, lengths_ref), (lambdas_hbm, lambdas_ref), (head_gain_hbm, head_gain_ref)]
    core = lax.rem(my_tp, 2)
    for taker, block_ref in ((1 - core, give_ref), (core, have_ref)):
        of_taker = pl.ds(taker * half, half)
        pairs += [(keys_hbm.at[of_taker], block_ref.at[0]), (values_hbm.at[of_taker], block_ref.at[1])]
    copies = [pltpu.make_async_copy(*pair, sems.at[i]) for i, pair in enumerate(pairs)]
    for copy in copies:
        copy.start()
    copies[0].wait()
    copies[1].wait()
    floats = tokens_ref[...].astype(jnp.float32)
    scaled = (floats * gain_ref[...]).astype(jnp.bfloat16)
    squares = jnp.sum(floats * floats, axis=1, keepdims=True)
    copies[2].wait()
    copies[3].wait()
    both = lax.dot_general(scaled, both_ref[...], CONTRACT_LAST, preferred_element_type=jnp.float32)
    if both.shape[1] < LANES:
        both = jnp.concatenate([both, jnp.zeros((seqs, LANES - both.shape[1]), jnp.float32)], axis=1)
    piece = (k_cols + v_cols) // n_kv
    both = jnp.concatenate([shifted(both[i : i + 1], i * piece) for i in range(seqs)], axis=0)
    lane = lane_of((seqs, LANES))
    row = lax.broadcasted_iota(jnp.int32, (seqs, LANES), 0)
    squares = jnp.where(lane == SQUARES_AT + row, squares, 0.0)
    queries = jnp.zeros((seqs, q_cols), jnp.float32)
    for i in range(CHUNKS):
        copies[4 + i].wait()
        queries += jnp.dot(
            scaled[:, i * rows : (i + 1) * rows], query_ref[chunks[i], :], preferred_element_type=jnp.float32
        )

    for i in range(seqs):
        row_scr[i // half, :, i % half * q_cols : (i % half + 1) * q_cols] = queries[i : i + 1]
    queries = [row_scr[c] for c in range(2)]

    def fill(v):
        slot = jnp.where(lane // piece == row, shifted(both, -v * piece), squares)
        slot = jnp.sum(slot, axis=0, keepdims=True)
        for t in range(n_tp):
            send_ref[v, t, :, : half * q_cols] = queries[t % 2]
            send_ref[v, t, :, half * q_cols :] = slot

    for_each(n_kv, fill)
    for copy in copies[4 + CHUNKS :]:
        copy.wait()
    own_block = lax.axis_index("kv") * n_tp + my_tp
    lane = lane_of((1, LANES))
    column_seq = lane // (2 * HEADS)
    for side, block in enumerate((own_block, own_block + 1 - 2 * core)):
        left = jnp.zeros((1, LANES), jnp.int32)
        for b in range(half):
            left = jnp.where(column_seq == b, lengths_ref[core * half + b] - block * pos_count, left)
        left_ref[side : side + 1, :] = left
    own_heads = lambdas_ref.shape[0]
    for g in range(own_heads):
        tail_ref[g : g + 1, :] = jnp.full((1, LANES), lambdas_ref[g], jnp.float32)
    tail_ref[own_heads : own_heads + 1, :] = head_gain_ref[...]


def attend(
    width,
    piece,
    left_ref,
    got_ref,
    have_ref,
    pair_ref,
    send_ref,
    q_scr,
    o_scr,
):
    n_kv, n_tp, half, _ = send_ref.shape
    pos_count = have_ref.shape[3]
    own_heads = HEADS // n_tp
    q_cols = own_heads * 2 * QK
    my_tp = lax.axis_index("tp")
    core = lax.rem(my_tp, 2)

    def add(v, sums):
        parts = [got_ref[v, t, :, : half * q_cols] for t in range(n_tp)] + [got_ref[v, my_tp, :, half * q_cols :]]
        return tuple(s + p for s, p in zip(sums, parts))

    zero = tuple(jnp.zeros((1, half * q_cols), jnp.float32) for _ in range(n_tp)) + (jnp.zeros((1, LANES), jnp.float32),)
    *totals, slot = lax.fori_loop(0, n_kv, add, zero, unroll=n_kv <= 8)
    inverses = [
        lax.rsqrt(slot[:, at : at + 1] / width + 1e-06) for at in range(SQUARES_AT, SQUARES_AT + 2 * half)
    ]
    lane = lane_of((1, LANES))
    scale = jnp.zeros((1, LANES), jnp.float32)
    for i, inverse in enumerate(inverses):
        scale = jnp.where(lane // piece == i, inverse, scale)
    own = jnp.concatenate([shifted(slot * scale, OWN_AT), jnp.zeros((half - 1, LANES), jnp.float32)], axis=0)
    per_seq = 2 * HEADS
    first_map = lane_of((1, q_cols)) % LANES < QK
    for b in range(half):
        inverse = jnp.where(core == 0, inverses[b], inverses[half + b])
        for t in range(n_tp):
            q = (totals[t][:, b * q_cols : (b + 1) * q_cols] * inverse).astype(jnp.bfloat16).astype(jnp.float32)
            maps = jnp.where(first_map, q, 0.0), jnp.where(first_map, 0.0, q)
            for g in range(own_heads):
                at = b * per_seq + 2 * (t * own_heads + g)
                for c in range(2):
                    q_scr[at + c : at + c + 1, :] = maps[c][:, g * LANES : (g + 1) * LANES]
    lane = lane_of((half, LANES))
    rows = 2 * GROUP
    pairs = [(b, h) for b in range(half) for h in range(KV_HEADS)]
    none = jnp.zeros((rows, LANES), jnp.bfloat16)
    queries = jnp.concatenate(
        [
            jnp.concatenate(
                [q_scr[i * rows : (i + 1) * rows, :].astype(jnp.bfloat16) if i == k else none for k in range(len(pairs))],
                axis=1,
            )
            for i in range(len(pairs))
        ],
        axis=0,
    )
    columns = queries.shape[0]
    row = lax.broadcasted_iota(jnp.int32, (pos_count, columns), 0)
    lives, scores = [], []
    for side in range(2):
        blocks = [(have_ref, pair_ref)[side][0, b, h] for b, h in pairs]
        keys = jnp.concatenate(blocks, axis=1)
        s = lax.dot_general(keys, queries, CONTRACT_LAST, preferred_element_type=jnp.float32) * QK ** (-0.5)
        live = row < left_ref[side : side + 1, :columns]
        lives.append(live)
        scores.append(jnp.where(live, s, NEG_FILL))
    peak = jnp.maximum(*(jnp.max(s, axis=0, keepdims=True) for s in scores))
    weights = [jnp.where(live, jnp.exp(s - peak), 0.0) for live, s in zip(lives, scores)]
    total = jnp.sum(weights[0], axis=0, keepdims=True) + jnp.sum(weights[1], axis=0, keepdims=True)
    some = total > 0.0
    total = jnp.where(some, total, 1.0)
    logs = jnp.where(some, peak + jnp.log(total), NEG_FILL)
    weights = jnp.concatenate(weights, axis=0) * (1.0 / total)
    if columns < LANES:
        weights, logs = (
            jnp.concatenate([x, jnp.zeros((x.shape[0], LANES - columns), jnp.float32)], axis=1) for x in (weights, logs)
        )
    weights = weights.T.astype(jnp.bfloat16)
    for i, (b, h) in enumerate(pairs):
        values = jnp.concatenate([have_ref[1, b, h], pair_ref[1, b, h]], axis=0)
        o_scr[i * rows : (i + 1) * rows, :] = jnp.dot(
            weights[i * rows : (i + 1) * rows], values, preferred_element_type=jnp.float32
        )
    per = 2 * own_heads
    logs = jnp.concatenate([shifted(logs, -b * per_seq) for b in range(half)], axis=0)
    parts = split3(logs)
    for t in range(n_tp):
        stats = own
        for k in reversed(range(3)):
            stats = jnp.where(lane < (k + 1) * per, shifted(parts[k], k * per - t * per), stats)
        stats = stats.astype(jnp.bfloat16)
        for j in range(per):
            o = o_scr[pl.ds(t * per + j, half, stride=per_seq), :].astype(jnp.bfloat16)
            for v in range(n_kv):
                send_ref[v, t, :, j * VD : (j + 1) * VD] = o
        for v in range(n_kv):
            send_ref[v, t, :, per * VD :] = stats


def finish(n_tp, piece, tail_ref, got_ref, weight_ref, out_ref, own_ref, log_scr, share_scr):
    count, half, _ = got_ref.shape
    own_heads = tail_ref.shape[0] - 1
    per = 2 * own_heads
    rows = count * half
    my_tp = lax.axis_index("tp")
    unroll = count <= 32

    def stage(d):
        log_scr[pl.ds(d * half, half), :] = got_ref[d, :, per * VD :].astype(jnp.float32)

    for_each(count, stage)
    logs = log_scr[...]
    logs = logs + shifted(logs, -per) + shifted(logs, -2 * per)
    logs = logs.reshape(rows // SUBLANES, SUBLANES, LANES)

    def over_sources(x, combine):
        by = 2 * half
        while by < SUBLANES:
            x = combine(x, pltpu.roll(x, by, 0))
            by *= 2
        return x

    peak = over_sources(jnp.max(logs, axis=0), jnp.maximum)
    shares = jnp.exp(logs - peak[None])
    shares = shares * (1.0 / over_sources(jnp.sum(shares, axis=0), jnp.add))[None]
    shares = shares.reshape(rows, LANES)
    for j in range(per):
        share_scr[j] = jnp.broadcast_to(shares[:, j : j + 1], (rows, LANES))
    ratios = []
    for j in range(per):

        def add(i, sums, j=j):
            return tuple(
                x
                + share_scr[j, pl.ds((2 * i + c) * half, half), :]
                * got_ref[2 * i + c, :, j * VD : (j + 1) * VD].astype(jnp.float32)
                for c, x in enumerate(sums)
            )

        zero = jnp.zeros((half, VD), jnp.float32)
        ratios.append(jnp.concatenate(lax.fori_loop(0, count // 2, add, (zero, zero), unroll=unroll), axis=0))
    heads = []
    for g in range(own_heads):
        mixed = ratios[2 * g] - tail_ref[g : g + 1, :] * ratios[2 * g + 1]
        scale = lax.rsqrt(jnp.mean(mixed * mixed, axis=1, keepdims=True) + 1e-06)
        heads.append((mixed * scale * tail_ref[own_heads : own_heads + 1, :]).astype(jnp.bfloat16))
    flattened = jnp.concatenate(heads, axis=1)
    out_ref[...] = jnp.dot(flattened, weight_ref[...], preferred_element_type=jnp.float32).astype(jnp.bfloat16)
    lane = lane_of((1, LANES))

    def collect(v, own):
        slot = log_scr[pl.ds((v * n_tp + my_tp) * half, 1), :]
        inside = (lane >= v * piece) & (lane < (v + 1) * piece)
        return tuple(
            jnp.where(inside, shifted(slot, v * piece - OWN_AT - i * piece), x) for i, x in enumerate(own)
        )

    zero = (jnp.zeros((1, LANES), jnp.float32),) * (2 * half)
    own = lax.fori_loop(0, count // n_tp, collect, zero, unroll=count // n_tp <= 8)
    own_ref[...] = jnp.concatenate(own, axis=0)


def body(
    tokens,
    norm_gain,
    query_weight,
    key_weight,
    value_weight,
    cache_keys,
    cache_values,
    lengths,
    lambdas,
    head_gain,
    output_weight,
):
    n_kv, n_tp = lax.axis_size("kv"), lax.axis_size("tp")
    everyone = ("kv", "tp")
    seqs = tokens.shape[0]
    half = seqs // 2
    own_heads = lambdas.shape[0]
    q_cols = query_weight.shape[1]
    k_cols, v_cols = key_weight.shape[1], value_weight.shape[1]
    pos_count = cache_keys.shape[2]
    width = tokens.shape[1] * n_kv
    first = half * q_cols + LANES
    piece = (k_cols + v_cols) // n_kv
    send, left, tail, give, have = pl.pallas_call(
        functools.partial(project, pos_count),
        out_shape=(
            jax.ShapeDtypeStruct((n_kv, n_tp, 1, first), jnp.float32),
            jax.ShapeDtypeStruct((2, LANES), jnp.int32),
            jax.ShapeDtypeStruct((own_heads + 1, LANES), jnp.float32),
            jax.ShapeDtypeStruct((2, half, *cache_keys.shape[1:]), cache_keys.dtype),
            jax.ShapeDtypeStruct((2, half, *cache_keys.shape[1:]), cache_keys.dtype),
        ),
        in_specs=[HBM] * 10,
        out_specs=(VMEM,) * 5,
        scratch_shapes=[
            pltpu.VMEM(tokens.shape, tokens.dtype),
            pltpu.VMEM((1, tokens.shape[1]), jnp.float32),
            pltpu.VMEM(query_weight.shape, query_weight.dtype),
            pltpu.VMEM((k_cols + v_cols, tokens.shape[1]), key_weight.dtype),
            pltpu.SMEM(lengths.shape, lengths.dtype),
            pltpu.SMEM(lambdas.shape, lambdas.dtype),
            pltpu.VMEM((1, LANES), jnp.float32),
            pltpu.VMEM((2, 1, half * q_cols), jnp.float32),
            pltpu.SemaphoreType.DMA((11 + CHUNKS,)),
        ],
        compiler_params=PARAMS,
    )(
        *(
            pltpu.with_memory_space_constraint(x, pltpu.HBM)
            for x in (
                tokens,
                norm_gain[None],
                query_weight,
                key_weight.T,
                value_weight.T,
                lengths,
                lambdas,
                head_gain[None],
                cache_keys,
                cache_values,
            )
        )
    )
    pair = lax.ppermute(give, "tp", [(i, i ^ 1) for i in range(n_tp)])
    got = lax.all_to_all(send.reshape(n_kv * n_tp, 1, first), everyone, 0, 0, tiled=True)
    got = got.reshape(n_kv, n_tp, 1, first)
    second = 2 * own_heads * VD + LANES
    rows = half * HEADS * 2
    send = pl.pallas_call(
        functools.partial(attend, width, piece),
        out_shape=jax.ShapeDtypeStruct((n_kv, n_tp, half, second), jnp.bfloat16),
        in_specs=[VMEM] * 4,
        out_specs=VMEM,
        compiler_params=PARAMS,
        scratch_shapes=[
            pltpu.VMEM((rows, LANES), jnp.float32),
            pltpu.VMEM((rows, LANES), jnp.float32),
        ],
    )(left, got, have, pair)
    got = lax.all_to_all(send.reshape(n_kv * n_tp, half, second), everyone, 0, 0, tiled=True)
    partial_out, own = pl.pallas_call(
        functools.partial(finish, n_tp, piece),
        out_shape=(
            jax.ShapeDtypeStruct((seqs, output_weight.shape[1]), jnp.bfloat16),
            jax.ShapeDtypeStruct((seqs, LANES), jnp.float32),
        ),
        in_specs=[VMEM] * 3,
        out_specs=(VMEM, VMEM),
        compiler_params=PARAMS,
        scratch_shapes=[
            pltpu.VMEM((n_kv * n_tp * half, LANES), jnp.float32),
            pltpu.VMEM((2 * own_heads, n_kv * n_tp * half, LANES), jnp.float32),
        ],
    )(tail, got, output_weight)
    new_keys = own[:, :k_cols].astype(jnp.bfloat16)
    new_values = own[:, k_cols : k_cols + v_cols].astype(jnp.bfloat16)
    out = partial_out.astype(jnp.float32)
    for step in sorted(range(1, n_tp), key=lambda i: i % 2 == 0):
        out = out + lax.ppermute(partial_out, "tp", [(i, i ^ step) for i in range(n_tp)]).astype(jnp.float32)
    return (out.astype(jnp.bfloat16), new_keys, new_values)


def solution(mesh):
    return jax.shard_map(
        body,
        mesh=mesh,
        in_specs=(
            P(None, "kv"),
            P("kv"),
            P("kv", "tp"),
            P("kv", "tp"),
            P("kv", "tp"),
            P(None, None, ("kv", "tp"), None),
            P(None, None, ("kv", "tp"), None),
            P(),
            P("tp"),
            P(),
            P("tp", "kv"),
        ),
        out_specs=(P(None, "kv"), P(None, "tp"), P(None, "tp")),
        check_vma=False,
    )
```

```python
import functools

import jax
import jax.numpy as jnp
from jax import lax
from jax.experimental import pallas as pl
from jax.experimental.pallas import tpu as pltpu
from jax.sharding import PartitionSpec as P

HEADS = 16
KV_HEADS = 2
QK = 64
VD = 128
LANES = 128
SUBLANES = 8
GROUP = HEADS // KV_HEADS
NEG_FILL = -1e30
VMEM = pl.BlockSpec(memory_space=pltpu.VMEM)
HBM = pl.BlockSpec(memory_space=pltpu.HBM)
PARAMS = pltpu.CompilerParams(vmem_limit_bytes=16 * 1024 * 1024)
CHUNKS = 2
SQUARES_AT = 96
OWN_AT = 64
CONTRACT_LAST = (((1,), (1,)), ((), ()))


def split3(x):
    high = x.astype(jnp.bfloat16).astype(jnp.float32)
    middle = (x - high).astype(jnp.bfloat16).astype(jnp.float32)
    low = x - high - middle
    return high, middle, low


def lane_of(shape):
    return lax.broadcasted_iota(jnp.int32, shape, 1)


def for_each(count, step):
    if count <= 32:
        for i in range(count):
            step(i)
    else:
        lax.fori_loop(0, count, lambda i, _: step(i), None)


def shifted(x, by):
    return pltpu.roll(x, lax.rem(by + 2 * LANES, LANES) if not isinstance(by, int) else by % LANES, 1)


def project(
    pos_count,
    tokens_hbm,
    gain_hbm,
    query_hbm,
    key_hbm,
    value_hbm,
    lengths_hbm,
    lambdas_hbm,
    head_gain_hbm,
    keys_hbm,
    values_hbm,
    send_ref,
    left_ref,
    tail_ref,
    give_ref,
    have_ref,
    tokens_ref,
    gain_ref,
    query_ref,
    both_ref,
    lengths_ref,
    lambdas_ref,
    head_gain_ref,
    row_scr,
    sems,
):
    n_kv, n_tp = send_ref.shape[:2]
    seqs = tokens_hbm.shape[0]
    half = seqs // 2
    q_cols = query_hbm.shape[1]
    k_cols, v_cols = key_hbm.shape[0], value_hbm.shape[0]
    my_tp = lax.axis_index("tp")
    rows = query_hbm.shape[0] // CHUNKS
    chunks = [pl.ds(i * rows, rows) for i in range(CHUNKS)]
    pairs = [
        (tokens_hbm, tokens_ref),
        (gain_hbm, gain_ref),
        (key_hbm, both_ref.at[pl.ds(0, k_cols)]),
        (value_hbm, both_ref.at[pl.ds(k_cols, v_cols)]),
    ]
    pairs += [(query_hbm.at[chunk], query_ref.at[chunk]) for chunk in chunks]
    pairs += [(lengths_hbm, lengths_ref), (lambdas_hbm, lambdas_ref), (head_gain_hbm, head_gain_ref)]
    core = lax.rem(my_tp, 2)
    for taker, block_ref in ((1 - core, give_ref), (core, have_ref)):
        of_taker = pl.ds(taker * half, half)
        pairs += [(keys_hbm.at[of_taker], block_ref.at[0]), (values_hbm.at[of_taker], block_ref.at[1])]
    copies = [pltpu.make_async_copy(*pair, sems.at[i]) for i, pair in enumerate(pairs)]
    for copy in copies:
        copy.start()
    copies[0].wait()
    copies[1].wait()
    floats = tokens_ref[...].astype(jnp.float32)
    scaled = (floats * gain_ref[...]).astype(jnp.bfloat16)
    squares = jnp.sum(floats * floats, axis=1, keepdims=True)
    copies[2].wait()
    copies[3].wait()
    both = lax.dot_general(both_ref[...], scaled, CONTRACT_LAST, preferred_element_type=jnp.float32).T
    if both.shape[1] < LANES:
        both = jnp.concatenate([both, jnp.zeros((seqs, LANES - both.shape[1]), jnp.float32)], axis=1)
    piece = (k_cols + v_cols) // n_kv
    both = jnp.concatenate([shifted(both[i : i + 1], i * piece) for i in range(seqs)], axis=0)
    lane = lane_of((seqs, LANES))
    row = lax.broadcasted_iota(jnp.int32, (seqs, LANES), 0)
    squares = jnp.where(lane == SQUARES_AT + row, squares, 0.0)
    queries = jnp.zeros((seqs, q_cols), jnp.float32)
    for i in range(CHUNKS):
        copies[4 + i].wait()
        queries += jnp.dot(
            scaled[:, i * rows : (i + 1) * rows], query_ref[chunks[i], :], preferred_element_type=jnp.float32
        )

    for i in range(seqs):
        row_scr[i // half, :, i % half * q_cols : (i % half + 1) * q_cols] = queries[i : i + 1]
    queries = [row_scr[c] for c in range(2)]

    def fill(v):
        slot = jnp.where(lane // piece == row, shifted(both, -v * piece), squares)
        slot = jnp.sum(slot, axis=0, keepdims=True)
        for t in range(n_tp):
            send_ref[v, t, :, : half * q_cols] = queries[t % 2]
            send_ref[v, t, :, half * q_cols :] = slot

    for_each(n_kv, fill)
    for copy in copies[4 + CHUNKS :]:
        copy.wait()
    own_block = lax.axis_index("kv") * n_tp + my_tp
    lane = lane_of((1, LANES))
    column_seq = lane // (2 * HEADS)
    for side, block in enumerate((own_block, own_block + 1 - 2 * core)):
        left = jnp.zeros((1, LANES), jnp.int32)
        for b in range(half):
            left = jnp.where(column_seq == b, lengths_ref[core * half + b] - block * pos_count, left)
        left_ref[side : side + 1, :] = left
    own_heads = lambdas_ref.shape[0]
    for g in range(own_heads):
        tail_ref[g : g + 1, :] = jnp.full((1, LANES), lambdas_ref[g], jnp.float32)
    tail_ref[own_heads : own_heads + 1, :] = head_gain_ref[...]


def attend(
    width,
    piece,
    left_ref,
    got_ref,
    have_ref,
    pair_ref,
    send_ref,
    q_scr,
    o_scr,
):
    n_kv, n_tp, half, _ = send_ref.shape
    pos_count = have_ref.shape[3]
    own_heads = HEADS // n_tp
    q_cols = own_heads * 2 * QK
    my_tp = lax.axis_index("tp")
    core = lax.rem(my_tp, 2)

    def add(v, sums):
        parts = [got_ref[v, t, :, : half * q_cols] for t in range(n_tp)] + [got_ref[v, my_tp, :, half * q_cols :]]
        return tuple(s + p for s, p in zip(sums, parts))

    zero = tuple(jnp.zeros((1, half * q_cols), jnp.float32) for _ in range(n_tp)) + (jnp.zeros((1, LANES), jnp.float32),)
    *totals, slot = lax.fori_loop(0, n_kv, add, zero, unroll=n_kv <= 8)
    inverses = [
        lax.rsqrt(slot[:, at : at + 1] / width + 1e-06) for at in range(SQUARES_AT, SQUARES_AT + 2 * half)
    ]
    lane = lane_of((1, LANES))
    scale = jnp.zeros((1, LANES), jnp.float32)
    for i, inverse in enumerate(inverses):
        scale = jnp.where(lane // piece == i, inverse, scale)
    own = jnp.concatenate([shifted(slot * scale, OWN_AT), jnp.zeros((half - 1, LANES), jnp.float32)], axis=0)
    per_seq = 2 * HEADS
    first_map = lane_of((1, q_cols)) % LANES < QK
    for b in range(half):
        inverse = jnp.where(core == 0, inverses[b], inverses[half + b])
        for t in range(n_tp):
            q = (totals[t][:, b * q_cols : (b + 1) * q_cols] * inverse).astype(jnp.bfloat16).astype(jnp.float32)
            maps = jnp.where(first_map, q, 0.0), jnp.where(first_map, 0.0, q)
            for g in range(own_heads):
                at = b * per_seq + 2 * (t * own_heads + g)
                for c in range(2):
                    q_scr[at + c : at + c + 1, :] = maps[c][:, g * LANES : (g + 1) * LANES]
    lane = lane_of((half, LANES))
    rows = 2 * GROUP
    pairs = [(b, h) for b in range(half) for h in range(KV_HEADS)]
    none = jnp.zeros((rows, LANES), jnp.bfloat16)
    queries = jnp.concatenate(
        [
            jnp.concatenate(
                [q_scr[i * rows : (i + 1) * rows, :].astype(jnp.bfloat16) if i == k else none for k in range(len(pairs))],
                axis=1,
            )
            for i in range(len(pairs))
        ],
        axis=0,
    )
    columns = queries.shape[0]
    row = lax.broadcasted_iota(jnp.int32, (pos_count, columns), 0)
    lives, scores = [], []
    for side in range(2):
        blocks = [(have_ref, pair_ref)[side][0, b, h] for b, h in pairs]
        keys = jnp.concatenate(blocks, axis=1)
        s = lax.dot_general(keys, queries, CONTRACT_LAST, preferred_element_type=jnp.float32) * QK ** (-0.5)
        live = row < left_ref[side : side + 1, :columns]
        lives.append(live)
        scores.append(jnp.where(live, s, NEG_FILL))
    peak = jnp.maximum(*(jnp.max(s, axis=0, keepdims=True) for s in scores))
    weights = [jnp.where(live, jnp.exp(s - peak), 0.0) for live, s in zip(lives, scores)]
    total = jnp.sum(weights[0], axis=0, keepdims=True) + jnp.sum(weights[1], axis=0, keepdims=True)
    some = total > 0.0
    total = jnp.where(some, total, 1.0)
    logs = jnp.where(some, peak + jnp.log(total), NEG_FILL)
    weights = jnp.concatenate(weights, axis=0) * (1.0 / total)
    if columns < LANES:
        weights, logs = (
            jnp.concatenate([x, jnp.zeros((x.shape[0], LANES - columns), jnp.float32)], axis=1) for x in (weights, logs)
        )
    weights = weights.T.astype(jnp.bfloat16)
    for i, (b, h) in enumerate(pairs):
        values = jnp.concatenate([have_ref[1, b, h], pair_ref[1, b, h]], axis=0)
        o_scr[i * rows : (i + 1) * rows, :] = jnp.dot(
            weights[i * rows : (i + 1) * rows], values, preferred_element_type=jnp.float32
        )
    per = 2 * own_heads
    logs = jnp.concatenate([shifted(logs, -b * per_seq) for b in range(half)], axis=0)
    parts = split3(logs)
    for t in range(n_tp):
        stats = own
        for k in reversed(range(3)):
            stats = jnp.where(lane < (k + 1) * per, shifted(parts[k], k * per - t * per), stats)
        stats = stats.astype(jnp.bfloat16)
        for j in range(per):
            o = o_scr[pl.ds(t * per + j, half, stride=per_seq), :].astype(jnp.bfloat16)
            for v in range(n_kv):
                send_ref[v, t, :, j * VD : (j + 1) * VD] = o
        for v in range(n_kv):
            send_ref[v, t, :, per * VD :] = stats


def finish(n_tp, piece, tail_ref, got_ref, weight_ref, out_ref, own_ref, log_scr, share_scr):
    count, half, _ = got_ref.shape
    own_heads = tail_ref.shape[0] - 1
    per = 2 * own_heads
    rows = count * half
    my_tp = lax.axis_index("tp")
    unroll = count <= 32

    def stage(d):
        log_scr[pl.ds(d * half, half), :] = got_ref[d, :, per * VD :].astype(jnp.float32)

    for_each(count, stage)
    logs = log_scr[...]
    logs = logs + shifted(logs, -per) + shifted(logs, -2 * per)
    logs = logs.reshape(rows // SUBLANES, SUBLANES, LANES)

    def over_sources(x, combine):
        by = 2 * half
        while by < SUBLANES:
            x = combine(x, pltpu.roll(x, by, 0))
            by *= 2
        return x

    peak = over_sources(jnp.max(logs, axis=0), jnp.maximum)
    shares = jnp.exp(logs - peak[None])
    shares = shares * (1.0 / over_sources(jnp.sum(shares, axis=0), jnp.add))[None]
    shares = shares.reshape(rows, LANES)
    for j in range(per):
        share_scr[j] = jnp.broadcast_to(shares[:, j : j + 1], (rows, LANES))
    ratios = []
    for j in range(per):

        def add(i, sums, j=j):
            return tuple(
                x
                + share_scr[j, pl.ds((2 * i + c) * half, half), :]
                * got_ref[2 * i + c, :, j * VD : (j + 1) * VD].astype(jnp.float32)
                for c, x in enumerate(sums)
            )

        zero = jnp.zeros((half, VD), jnp.float32)
        ratios.append(jnp.concatenate(lax.fori_loop(0, count // 2, add, (zero, zero), unroll=unroll), axis=0))
    heads = []
    for g in range(own_heads):
        mixed = ratios[2 * g] - tail_ref[g : g + 1, :] * ratios[2 * g + 1]
        scale = lax.rsqrt(jnp.mean(mixed * mixed, axis=1, keepdims=True) + 1e-06)
        heads.append((mixed * scale * tail_ref[own_heads : own_heads + 1, :]).astype(jnp.bfloat16))
    flattened = jnp.concatenate(heads, axis=1)
    out_ref[...] = jnp.dot(flattened, weight_ref[...], preferred_element_type=jnp.float32).astype(jnp.bfloat16)
    lane = lane_of((1, LANES))

    def collect(v, own):
        slot = log_scr[pl.ds((v * n_tp + my_tp) * half, 1), :]
        inside = (lane >= v * piece) & (lane < (v + 1) * piece)
        return tuple(
            jnp.where(inside, shifted(slot, v * piece - OWN_AT - i * piece), x) for i, x in enumerate(own)
        )

    zero = (jnp.zeros((1, LANES), jnp.float32),) * (2 * half)
    own = lax.fori_loop(0, count // n_tp, collect, zero, unroll=count // n_tp <= 8)
    own_ref[...] = jnp.concatenate(own, axis=0)


def body(
    tokens,
    norm_gain,
    query_weight,
    key_weight,
    value_weight,
    cache_keys,
    cache_values,
    lengths,
    lambdas,
    head_gain,
    output_weight,
):
    n_kv, n_tp = lax.axis_size("kv"), lax.axis_size("tp")
    everyone = ("kv", "tp")
    seqs = tokens.shape[0]
    half = seqs // 2
    own_heads = lambdas.shape[0]
    q_cols = query_weight.shape[1]
    k_cols, v_cols = key_weight.shape[1], value_weight.shape[1]
    pos_count = cache_keys.shape[2]
    width = tokens.shape[1] * n_kv
    first = half * q_cols + LANES
    piece = (k_cols + v_cols) // n_kv
    send, left, tail, give, have = pl.pallas_call(
        functools.partial(project, pos_count),
        out_shape=(
            jax.ShapeDtypeStruct((n_kv, n_tp, 1, first), jnp.float32),
            jax.ShapeDtypeStruct((2, LANES), jnp.int32),
            jax.ShapeDtypeStruct((own_heads + 1, LANES), jnp.float32),
            jax.ShapeDtypeStruct((2, half, *cache_keys.shape[1:]), cache_keys.dtype),
            jax.ShapeDtypeStruct((2, half, *cache_keys.shape[1:]), cache_keys.dtype),
        ),
        in_specs=[HBM] * 10,
        out_specs=(VMEM,) * 5,
        scratch_shapes=[
            pltpu.VMEM(tokens.shape, tokens.dtype),
            pltpu.VMEM((1, tokens.shape[1]), jnp.float32),
            pltpu.VMEM(query_weight.shape, query_weight.dtype),
            pltpu.VMEM((k_cols + v_cols, tokens.shape[1]), key_weight.dtype),
            pltpu.SMEM(lengths.shape, lengths.dtype),
            pltpu.SMEM(lambdas.shape, lambdas.dtype),
            pltpu.VMEM((1, LANES), jnp.float32),
            pltpu.VMEM((2, 1, half * q_cols), jnp.float32),
            pltpu.SemaphoreType.DMA((11 + CHUNKS,)),
        ],
        compiler_params=PARAMS,
    )(
        *(
            pltpu.with_memory_space_constraint(x, pltpu.HBM)
            for x in (
                tokens,
                norm_gain[None],
                query_weight,
                key_weight.T,
                value_weight.T,
                lengths,
                lambdas,
                head_gain[None],
                cache_keys,
                cache_values,
            )
        )
    )
    pair = lax.ppermute(give, "tp", [(i, i ^ 1) for i in range(n_tp)])
    got = lax.all_to_all(send.reshape(n_kv * n_tp, 1, first), everyone, 0, 0, tiled=True)
    got = got.reshape(n_kv, n_tp, 1, first)
    second = 2 * own_heads * VD + LANES
    rows = half * HEADS * 2
    send = pl.pallas_call(
        functools.partial(attend, width, piece),
        out_shape=jax.ShapeDtypeStruct((n_kv, n_tp, half, second), jnp.bfloat16),
        in_specs=[VMEM] * 4,
        out_specs=VMEM,
        compiler_params=PARAMS,
        scratch_shapes=[
            pltpu.VMEM((rows, LANES), jnp.float32),
            pltpu.VMEM((rows, LANES), jnp.float32),
        ],
    )(left, got, have, pair)
    got = lax.all_to_all(send.reshape(n_kv * n_tp, half, second), everyone, 0, 0, tiled=True)
    partial_out, own = pl.pallas_call(
        functools.partial(finish, n_tp, piece),
        out_shape=(
            jax.ShapeDtypeStruct((seqs, output_weight.shape[1]), jnp.bfloat16),
            jax.ShapeDtypeStruct((seqs, LANES), jnp.float32),
        ),
        in_specs=[VMEM] * 3,
        out_specs=(VMEM, VMEM),
        compiler_params=PARAMS,
        scratch_shapes=[
            pltpu.VMEM((n_kv * n_tp * half, LANES), jnp.float32),
            pltpu.VMEM((2 * own_heads, n_kv * n_tp * half, LANES), jnp.float32),
        ],
    )(tail, got, output_weight)
    new_keys = own[:, :k_cols].astype(jnp.bfloat16)
    new_values = own[:, k_cols : k_cols + v_cols].astype(jnp.bfloat16)
    out = partial_out.astype(jnp.float32)
    for step in sorted(range(1, n_tp), key=lambda i: i % 2 == 0):
        out = out + lax.ppermute(partial_out, "tp", [(i, i ^ step) for i in range(n_tp)]).astype(jnp.float32)
    return (out.astype(jnp.bfloat16), new_keys, new_values)


def solution(mesh):
    return jax.shard_map(
        body,
        mesh=mesh,
        in_specs=(
            P(None, "kv"),
            P("kv"),
            P("kv", "tp"),
            P("kv", "tp"),
            P("kv", "tp"),
            P(None, None, ("kv", "tp"), None),
            P(None, None, ("kv", "tp"), None),
            P(),
            P("tp"),
            P(),
            P("tp", "kv"),
        ),
        out_specs=(P(None, "kv"), P(None, "tp"), P(None, "tp")),
        check_vma=False,
    )
```
